256 devices in a mesh: ep: 32 (over z, x), tp: 8 (over y, core).
Axes of the slice: x: 4, y: 4, z: 8, core: 2. Of those that a mesh axis runs over, the one named last changes fastest.
Arguments:
- mixer_input: bfloat16 [4096, 2048], P('ep'), may hold values from -6 to 6
- mixer_gain: bfloat16 [2048], replicated, may hold values from 0.099609375 to 1.8984375
- query_matrix: bfloat16 [2048, 2048], P(None, 'tp'), may hold values from -0.125 to 0.125
- key_matrix: bfloat16 [2048, 2048], P(None, 'tp'), may hold values from -0.125 to 0.125
- value_matrix: bfloat16 [2048, 2048], P(None, 'tp'), may hold values from -0.125 to 0.125
- decay_down_factor: bfloat16 [2048, 64], replicated, may hold values from -0.125 to 0.125
- decay_up_factor: bfloat16 [64, 2048], P(None, 'tp'), may hold values from -1.1953125 to 1.1953125
- decay_bias_base: float32 [2048], P('tp'), may hold values from -16 to 0
- decay_shift: float32 [4096, 2048], P('ep', 'tp'), may hold values from -1.5 to 1.5
- decay_spike: float32 [4096, 2048], P('ep', 'tp'), may hold values from -1.4 to 0
- correction_rate_down: bfloat16 [2048, 64], replicated, may hold values from -0.125 to 0.125
- correction_rate_up: bfloat16 [64, 2048], P(None, 'tp'), may hold values from -1.1953125 to 1.1953125
- correction_rate_base: float32 [2048], P('tp'), may hold values from -8 to 1
- head_norm_gain: bfloat16 [2048], P('tp'), may hold values from 0.099609375 to 1.8984375
- output_weight: bfloat16 [2048, 2048], P('tp'), may hold values from -0.125 to 0.125
- feedforward_input: bfloat16 [8192, 2048], P(('ep', 'tp')), may hold values from -6 to 6
- feedforward_gain: bfloat16 [2048], replicated, may hold values from 0.099609375 to 1.8984375
- routed_expert_index: int32 [8192, 2], P('ep'), may hold values from 0 to 63, all different within a row; in each aligned block of 32 rows (0 to 31, 32 to 63, ...) at most 2 rows name the same one
- routed_expert_weight: float32 [8192, 2], P(('ep', 'tp')), may hold values from 0.3 to 2.5
- expert_gate_weight: bfloat16 [64, 2048, 1024], P('ep', None, 'tp'), may hold values from -0.125 to 0.125
- expert_up_weight: bfloat16 [64, 2048, 1024], P('ep', None, 'tp'), may hold values from -0.125 to 0.125
- expert_down_weight: bfloat16 [64, 1024, 2048], P('ep', 'tp'), may hold values from -0.1875 to 0.1875
- shared_gate_weight: bfloat16 [2048, 1024], P(None, 'tp'), may hold values from -0.125 to 0.125
- shared_up_weight: bfloat16 [2048, 1024], P(None, 'tp'), may hold values from -0.125 to 0.125
- shared_down_weight: bfloat16 [1024, 2048], P('tp'), may hold values from -0.1875 to 0.1875
Outputs:
- mixed_a: bfloat16 [4096, 2048], P(('ep', 'tp'))
- mixed_b: bfloat16 [8192, 2048], P(('ep', 'tp'))
The draws below stay inside these ranges and needn't reach their ends.
Inputs may be any that keep to these rules, and one draw needn't show every extreme that they name: `routed_expert_index`: in each aligned block of 32 rows (the rows of one device) a row names 2 different experts and no expert is named more than 2 times; in every draw some block names some expert exactly 2 times.
All inputs are finite; a program needn't handle non-finite values.
Results may differ from the reference program's by a relative error of at most 0.017.
Values may be sent and summed in bfloat16 or wider, within the bound.
A program may use at most 128 MiB of HBM per device.

```python
import math
import jax
import jax.numpy as jnp
import numpy as np
from jax import lax

MODEL_DIMENSION = 2048
MIXER_HEADS = 32
HEAD = 64
DECAY_RANK = 64
FE = 1024
TOP = 2
SPAN = 32
ROWS_A = 128
MIXER_CHANNELS = 2048
EXPERTS = 64
TOKB = 32
CAP = 2
FIRST_TOKENS = 4096
TOKENS_B = 8192
N_EP = 32
N_TP = 8


def slow_heads(key):
    shuffled = jax.random.permutation(jax.random.fold_in(key, 11), MIXER_HEADS)
    keep_count = MIXER_HEADS // 2
    return jnp.repeat(shuffled < keep_count, HEAD)


def draw_decay_bias_base(key, part):
    slow = slow_heads(key)
    noise = jax.random.uniform(jax.random.fold_in(key, 1), (MIXER_HEADS * HEAD,), jnp.float32, -0.5, 0.5)
    slow_level = math.log(0.3 / FIRST_TOKENS) + 0.5
    fast_level = math.log(1.0 / 40.0) + 0.5
    return jnp.where(slow, slow_level, fast_level) + noise


def draw_correction_rate_base(key, part):
    slow = slow_heads(key)
    noise = jax.random.uniform(jax.random.fold_in(key, 2), (MIXER_HEADS * HEAD,), jnp.float32, -0.5, 0.5)
    return jnp.where(slow, -7.0 + noise, 2.0 * noise)


def draw_decay_shift(key, part):
    channel_count = MIXER_HEADS * HEAD
    segments = FIRST_TOKENS // ROWS_A
    spans = FIRST_TOKENS // SPAN
    coarse = jax.random.uniform(jax.random.fold_in(key, 3), (segments, channel_count), jnp.float32, -0.7, 0.7)
    detail = jax.random.uniform(jax.random.fold_in(key, 4), (spans, channel_count), jnp.float32, -0.4, 0.4)
    return jnp.repeat(coarse, ROWS_A, axis=0) + jnp.repeat(detail, SPAN, axis=0)


def draw_decay_spike(key, part):
    channel_count = MIXER_HEADS * HEAD
    spike_count = 6
    slot_places = jax.random.randint(jax.random.fold_in(key, 5), (spike_count, MIXER_HEADS), 0, FIRST_TOKENS)
    layer_depth = jax.random.uniform(jax.random.fold_in(key, 6), (spike_count, channel_count), jnp.float32, math.log(0.5), math.log(0.8))
    positions = jnp.arange(FIRST_TOKENS, dtype=jnp.int32)
    result = jnp.zeros((FIRST_TOKENS, channel_count), jnp.float32)
    for item_number in range(spike_count):
        hits = (positions[:, None] == jnp.repeat(slot_places[item_number], HEAD)[None, :]).astype(jnp.float32)
        result = result + hits * layer_depth[item_number][None, :]
    return result


def level_of(key, shape, shards, smallest, top_value):
    factor_of = 1.0
    for axis_at, shards_of in shards:
        heights = jax.random.uniform(jax.random.fold_in(jax.random.fold_in(key, 6), axis_at), (shards_of,), jnp.float32, smallest / len(shards), top_value / len(shards))
        factor_of = factor_of * jnp.repeat(jnp.exp(heights), shape[axis_at] // shards_of).reshape((-1,) + (1,) * (len(shape) - 1 - axis_at))
    return factor_of


def deal_out(own_key, own, number, rows, amount, top, limit, slope):
    order = jax.random.permutation(own_key, amount)
    crowded, ordinary = portions_of(amount, rows * top, limit, slope, True), portions_of(amount, rows * top, limit, slope, False)
    places = jnp.arange(amount)

    def named(lengths, rotation):
        used = int((lengths > 0).sum())
        fixed = max(1, used // 4)
        shifted = fixed + (places - fixed + rotation * (used - fixed)) % max(1, amount - fixed)
        return jnp.zeros((amount,), jnp.int32).at[order[jnp.where(places < fixed, places, shifted)]].set(jnp.asarray(lengths, jnp.int32))

    lengths = jnp.where(number % 4 == 0, named(crowded, number // 4), named(ordinary, number - number // 4 - 1))
    mixed = jax.random.permutation(jax.random.fold_in(own, 3), amount)
    giver, taker = mixed[0:amount // 2 * 2:2], mixed[1:amount // 2 * 2:2]
    margin = jnp.minimum(lengths[giver] - 1, limit - lengths[taker]) // 2
    margin = jnp.where((giver == order[0]) | (taker == order[0]) | (lengths[taker] == 0), 0, jnp.maximum(margin, 0))
    shifted = jax.random.randint(jax.random.fold_in(own, 4), (amount // 2,), 0, 1 << 20) % (margin + 1)
    lengths = lengths.at[giver].add(-shifted).at[taker].add(shifted)
    labels = jnp.searchsorted(jnp.cumsum(lengths), jnp.arange(rows * top), side="right").astype(jnp.int32)
    table = labels.reshape(top, rows).T
    table = table[jax.random.permutation(jax.random.fold_in(own, 1), rows)]
    rotation = jax.random.randint(jax.random.fold_in(own, 2), (rows, 1), 0, top)
    return jnp.take_along_axis(table, (jnp.arange(top)[None, :] + rotation) % top, axis=1)


def portions_of(count, total, limit, lean, full):
    loads = [(1 << 20) // math.isqrt(rank ** lean) + 1 for rank in range(1, count + 1)]
    largest = limit if full else min(limit, max(-(-total // count), total * loads[0] // sum(loads)))
    least = 1 if total - largest >= count - 1 else 0
    holding, surplus = [largest] + [least] * (count - 1), total - largest - least * (count - 1)
    while surplus > 0:
        movable = [i for i in range(1, count) if holding[i] < largest] or [i for i in range(1, count) if holding[i] < limit]
        mass, left = sum([loads[i] for i in movable]), surplus
        for i in movable:
            addition = min(limit - holding[i], max(1, left * loads[i] // mass), surplus)
            holding[i] = holding[i] + addition
            surplus = surplus - addition
    return np.array(holding)


def scatter_about(rng, extent, spread, bound, split=(), kind=jnp.bfloat16):
    factor_of = level_of(rng, extent, split, -0.22, 0.18) if split else 1.0
    values = jax.random.normal(rng, extent, jnp.float32) * spread * factor_of
    return jnp.minimum(jnp.maximum(values, -bound), bound).astype(kind)


def setup_inputs(seed: int = 0) -> dict:
    arg_keys = jax.random.split(jax.random.key(seed), 26)
    mixer_input = scatter_about(arg_keys[0], (FIRST_TOKENS, MODEL_DIMENSION), 1.0, 6.0, ((0, 32),))
    mixer_gain = jnp.clip(1.0 + 0.18 * jax.random.normal(arg_keys[1], (MODEL_DIMENSION,), jnp.float32), 0.099609375, 1.8984375).astype(jnp.bfloat16)
    query_matrix = scatter_about(arg_keys[2], (MODEL_DIMENSION, MIXER_CHANNELS), MODEL_DIMENSION ** -0.5, 0.125, ((1, 8),))
    key_matrix = scatter_about(arg_keys[3], (MODEL_DIMENSION, MIXER_CHANNELS), MODEL_DIMENSION ** -0.5, 0.125, ((1, 8),))
    value_matrix = scatter_about(arg_keys[4], (MODEL_DIMENSION, MIXER_CHANNELS), MODEL_DIMENSION ** -0.5, 0.125, ((1, 8),))
    decay_down_factor = scatter_about(arg_keys[5], (MODEL_DIMENSION, DECAY_RANK), MODEL_DIMENSION ** -0.5, 0.125)
    decay_up_factor = scatter_about(arg_keys[6], (DECAY_RANK, MIXER_CHANNELS), 0.2, 1.1953125, ((1, 8),))
    decay_bias_base = draw_decay_bias_base(jax.random.fold_in(arg_keys[25], 71), 0)
    decay_shift = draw_decay_shift(jax.random.fold_in(arg_keys[25], 71), 0)
    decay_spike = draw_decay_spike(jax.random.fold_in(arg_keys[25], 71), 0)
    correction_rate_down = scatter_about(arg_keys[10], (MODEL_DIMENSION, DECAY_RANK), MODEL_DIMENSION ** -0.5, 0.125)
    correction_rate_up = scatter_about(arg_keys[11], (DECAY_RANK, MIXER_CHANNELS), 0.2, 1.1953125, ((1, 8),))
    correction_rate_base = draw_correction_rate_base(jax.random.fold_in(arg_keys[25], 71), 0)
    head_norm_gain = jnp.clip(1.0 + 0.18 * jax.random.normal(arg_keys[13], (MIXER_CHANNELS,), jnp.float32), 0.099609375, 1.8984375).astype(jnp.bfloat16)
    output_weight = scatter_about(arg_keys[14], (MIXER_CHANNELS, MODEL_DIMENSION), MIXER_CHANNELS ** -0.5, 0.125, ((0, 8),))
    feedforward_input = scatter_about(arg_keys[15], (TOKENS_B, MODEL_DIMENSION), 1.0, 6.0, ((0, 256),))
    feedforward_gain = jnp.clip(1.0 + 0.18 * jax.random.normal(arg_keys[16], (MODEL_DIMENSION,), jnp.float32), 0.099609375, 1.8984375).astype(jnp.bfloat16)
    routed_expert_index_keys = jax.random.split(jax.random.fold_in(arg_keys[17], 1), TOKENS_B // TOKB)
    routed_expert_index_turns = jax.random.permutation(jax.random.fold_in(arg_keys[17], 3), TOKENS_B // TOKB)
    routed_expert_index = jax.vmap(lambda own, number: deal_out(jax.random.fold_in(arg_keys[17], 2), own, number, TOKB, EXPERTS, TOP, CAP, 1))(routed_expert_index_keys, routed_expert_index_turns).reshape((TOKENS_B, TOP))
    routed_expert_weight = jnp.clip(jnp.exp(math.log(2.5) - 2.1202635 * jax.random.uniform(arg_keys[18], (TOKENS_B, TOP), jnp.float32) ** level_of(arg_keys[18], (TOKENS_B, TOP), ((0, 256),), -0.2, 0.2)), 0.3, 2.5)
    expert_gate_weight = scatter_about(arg_keys[19], (EXPERTS, MODEL_DIMENSION, FE), MODEL_DIMENSION ** -0.5, 0.125, ((0, 32), (2, 8)))
    expert_up_weight = scatter_about(arg_keys[20], (EXPERTS, MODEL_DIMENSION, FE), MODEL_DIMENSION ** -0.5, 0.125, ((0, 32), (2, 8)))
    expert_down_weight = scatter_about(arg_keys[21], (EXPERTS, FE, MODEL_DIMENSION), FE ** -0.5, 0.1875, ((0, 32), (1, 8)))
    shared_gate_weight = scatter_about(arg_keys[22], (MODEL_DIMENSION, FE), MODEL_DIMENSION ** -0.5, 0.125, ((1, 8),))
    shared_up_weight = scatter_about(arg_keys[23], (MODEL_DIMENSION, FE), MODEL_DIMENSION ** -0.5, 0.125, ((1, 8),))
    shared_down_weight = scatter_about(arg_keys[24], (FE, MODEL_DIMENSION), FE ** -0.5, 0.1875, ((0, 8),))
    return {"mixer_input": mixer_input, "mixer_gain": mixer_gain, "query_matrix": query_matrix, "key_matrix": key_matrix, "value_matrix": value_matrix, "decay_down_factor": decay_down_factor, "decay_up_factor": decay_up_factor, "decay_bias_base": decay_bias_base, "decay_shift": decay_shift, "decay_spike": decay_spike, "correction_rate_down": correction_rate_down, "correction_rate_up": correction_rate_up, "correction_rate_base": correction_rate_base, "head_norm_gain": head_norm_gain, "output_weight": output_weight, "feedforward_input": feedforward_input, "feedforward_gain": feedforward_gain, "routed_expert_index": routed_expert_index, "routed_expert_weight": routed_expert_weight, "expert_gate_weight": expert_gate_weight, "expert_up_weight": expert_up_weight, "expert_down_weight": expert_down_weight, "shared_gate_weight": shared_gate_weight, "shared_up_weight": shared_up_weight, "shared_down_weight": shared_down_weight}


highest = lax.Precision.HIGHEST
norm_eps = 1e-06
group_eps = 0.00064
unit_eps = 1e-06

def rms_rows(matrix, gain):
    values = matrix.astype(jnp.float32)
    scaled = values * lax.rsqrt(lax.optimization_barrier(jnp.mean(values * values, axis=-1, keepdims=True)) + norm_eps)
    return (scaled * gain.astype(jnp.float32)).astype(jnp.bfloat16)

def mixer_channel_rows(normed_rows, query_matrix, key_matrix, value_matrix, decay_down_factor, decay_up_factor, decay_bias_base, decay_shift, decay_spike, correction_rate_down, correction_rate_up, correction_rate_base):
    row_count = normed_rows.shape[0]
    head_count = query_matrix.shape[1] // HEAD

    def by_heads(matrix):
        return matrix.reshape(row_count, head_count, HEAD)
    query_matrix_rows = jnp.dot(normed_rows, query_matrix, preferred_element_type=jnp.float32)
    key_matrix_rows = jnp.dot(normed_rows, key_matrix, preferred_element_type=jnp.float32)
    value_matrix_rows = jnp.dot(normed_rows, value_matrix, preferred_element_type=jnp.float32)
    decay_low = jnp.tanh(jnp.dot(normed_rows, decay_down_factor, preferred_element_type=jnp.float32)).astype(jnp.bfloat16)
    decay_logits = decay_bias_base + jnp.dot(decay_low, decay_up_factor, preferred_element_type=jnp.float32) + decay_shift
    logarithm_decay = decay_spike - jnp.exp(-jax.nn.softplus(-decay_logits) - 0.5)
    iclr_low = jnp.dot(normed_rows, correction_rate_down, preferred_element_type=jnp.float32).astype(jnp.bfloat16)
    learning = jax.nn.sigmoid(correction_rate_base + jnp.dot(iclr_low, correction_rate_up, preferred_element_type=jnp.float32))
    key_matrix_rows = by_heads(key_matrix_rows)
    unit_keys = key_matrix_rows * lax.rsqrt(lax.optimization_barrier(jnp.sum(key_matrix_rows * key_matrix_rows, axis=-1, keepdims=True)) + unit_eps)
    return (by_heads(query_matrix_rows), key_matrix_rows, by_heads(value_matrix_rows), -unit_keys, unit_keys * by_heads(learning), by_heads(logarithm_decay))

def head_norm(outputs, gain):
    row_mean = lax.optimization_barrier(jnp.mean(outputs, axis=-1, keepdims=True))
    centered = outputs - row_mean
    row_var = lax.optimization_barrier(jnp.mean(centered * centered, axis=-1, keepdims=True))
    scaled = (centered * lax.rsqrt(row_var + group_eps)).reshape(outputs.shape[0], -1)
    return (scaled * gain.astype(jnp.float32)).astype(jnp.bfloat16)

def reference(mixer_input, mixer_gain, query_matrix, key_matrix, value_matrix, decay_down_factor, decay_up_factor, decay_bias_base, decay_shift, decay_spike, correction_rate_down, correction_rate_up, correction_rate_base, head_norm_gain, output_weight, feedforward_input, feedforward_gain, routed_expert_index, routed_expert_weight, expert_gate_weight, expert_up_weight, expert_down_weight, shared_gate_weight, shared_up_weight, shared_down_weight):
    normed_first = rms_rows(mixer_input, mixer_gain)
    query_matrix_rows, key_matrix_rows, value_matrix_rows, erase_vector, write_vector, logarithm_decay = mixer_channel_rows(normed_first, query_matrix, key_matrix, value_matrix, decay_down_factor, decay_up_factor, decay_bias_base, decay_shift, decay_spike, correction_rate_down, correction_rate_up, correction_rate_base)
    head_count = query_matrix_rows.shape[1]

    def advance(carried, inputs):
        query_t, key_t, value_t, erase_t, write_t, decay_t = inputs
        held = jnp.einsum('hvk,hk->hv', carried, erase_t, precision=highest)
        carried = carried * jnp.exp(decay_t)[:, None, :] + held[:, :, None] * write_t[:, None, :] + value_t[:, :, None] * key_t[:, None, :]
        return (carried, jnp.einsum('hvk,hk->hv', carried, query_t, precision=highest))
    initial = jnp.zeros((head_count, HEAD, HEAD), jnp.float32)
    _, head_out = lax.scan(advance, initial, (query_matrix_rows, key_matrix_rows, value_matrix_rows, erase_vector, write_vector, logarithm_decay))
    mixed_rows = head_norm(head_out, head_norm_gain)
    mixed_a = jnp.dot(mixed_rows, output_weight, preferred_element_type=jnp.float32).astype(jnp.bfloat16)
    normed_b = rms_rows(feedforward_input, feedforward_gain)
    total = normed_b.shape[0]
    model_width = normed_b.shape[1]
    padded = jnp.concatenate([normed_b, jnp.zeros((1, model_width), jnp.bfloat16)], axis=0)
    flat_ids = routed_expert_index.reshape(-1)
    most = N_EP * N_TP * CAP
    slice_width = FE // N_TP

    def one_expert(expert):
        picked = jnp.nonzero(flat_ids == expert, size=most, fill_value=total * TOP)[0].astype(jnp.int32)
        chosen = padded[picked // TOP]
        gate_out = jnp.dot(chosen, expert_gate_weight[expert], preferred_element_type=jnp.float32)
        up_out = jnp.dot(chosen, expert_up_weight[expert], preferred_element_type=jnp.float32)
        hidden = (jax.nn.silu(gate_out) * up_out).astype(jnp.bfloat16)
        pieces = hidden.astype(jnp.float32).reshape(most, N_TP, slice_width)
        down_blocks = expert_down_weight[expert].astype(jnp.float32).reshape(N_TP, slice_width, model_width)
        partial_value = jnp.einsum('rtf,tfd->trd', pieces, down_blocks)
        rounded = lax.optimization_barrier(partial_value.astype(jnp.bfloat16))
        summed = lax.optimization_barrier(jnp.sum(rounded.astype(jnp.float32), axis=0))
        return (summed.astype(jnp.bfloat16), picked)
    expert_out, picks = lax.map(one_expert, jnp.arange(EXPERTS, dtype=jnp.int32))
    placed = jnp.zeros((total * TOP + 1, model_width), jnp.bfloat16)
    placed = placed.at[picks.reshape(-1)].set(expert_out.reshape(-1, model_width))
    per_choice = placed[:total * TOP].reshape(total, TOP, model_width).astype(jnp.float32)
    routed = jnp.einsum('rk,rkd->rd', routed_expert_weight, per_choice, precision=highest)
    shared_hidden = (jax.nn.silu(jnp.dot(normed_b, shared_gate_weight, preferred_element_type=jnp.float32)) * jnp.dot(normed_b, shared_up_weight, preferred_element_type=jnp.float32)).astype(jnp.bfloat16)
    shared = jnp.zeros((total, model_width), jnp.float32)
    for block in range(N_TP):
        partial_value = jnp.dot(shared_hidden[:, block * slice_width:(block + 1) * slice_width], shared_down_weight[block * slice_width:(block + 1) * slice_width], preferred_element_type=jnp.float32)
        shared = shared + lax.optimization_barrier(partial_value.astype(jnp.bfloat16)).astype(jnp.float32)
    mixed_b = (routed + shared).astype(jnp.bfloat16)
    return (mixed_a, mixed_b)
```

```python
import jax
import jax.numpy as jnp
from jax import lax
from jax.experimental import pallas as pl
from jax.experimental.pallas import tpu as pltpu
from jax.sharding import Mesh
from jax.sharding import PartitionSpec as P

MESH = pl.DeviceIdType.MESH
BF, F32 = jnp.bfloat16, jnp.float32
norm_eps = 1e-06
group_eps = 0.00064
unit_eps = 1e-06
ROOT = 0.6065306597126334

HEADS = 4
HEAD = 64
SPAN = 32
ROWS = 128
TOK = 32
CHUNKS = 4
HALF = 1024
DZ = (0, 1, 7, 2, 6, 3, 5, 4)


def iota(shape, dim):
    return lax.broadcasted_iota(jnp.int32, shape, dim)


def dot(a, b, dims=((1,), (0,))):
    return lax.dot_general(a.astype(BF), b.astype(BF), (dims, ((), ())), preferred_element_type=F32)


def split(a):
    high = a.astype(BF)
    return high, (a - high.astype(F32)).astype(BF)


def dot3(a, b):
    ah, al = split(a)
    bh, bl = split(b)
    return dot(ah, bh) + (dot(ah, bl) + dot(al, bh))


def dot_exact_left(a, b):
    bh, rest = b.astype(BF), None
    rest = b - bh.astype(F32)
    bm = rest.astype(BF)
    bl = (rest - bm.astype(F32)).astype(BF)
    return dot(a, bh) + (dot(a, bm) + dot(a, bl))


def dot_exact_right(a, b):
    ah = a.astype(BF)
    rest = a - ah.astype(F32)
    am = rest.astype(BF)
    al = (rest - am.astype(F32)).astype(BF)
    return dot(ah, b) + (dot(am, b) + dot(al, b))


def sigmoid(u):
    e = jnp.exp(-jnp.abs(u))
    return jnp.where(u >= 0, 1.0, e) / (1.0 + e)


def rms(values, gain):
    values = values.astype(F32)
    scaled = values * lax.rsqrt(jnp.mean(values * values, axis=-1, keepdims=True) + norm_eps)
    return (scaled * gain.astype(F32)).astype(BF)


def ones_where(mask, kind=BF):
    return jnp.where(mask, 1.0, 0.0).astype(kind)


def compose(later, earlier):
    lane = iota(later.shape, 1)
    return dot3(later[:, :HEAD], earlier) + jnp.where(lane >= HEAD, later, 0.0)


def quarter_rows(matrix):
    return jnp.concatenate([matrix[:, 512 * q : 512 * (q + 1)] for q in range(4)], axis=0)


def quarter_lanes(matrix, rows):
    return jnp.concatenate([matrix[rows * q : rows * (q + 1)] for q in range(4)], axis=1)


def kernel(
    xa, gain_a, wq, wk, wv, decay_down, decay_up, decay_bias, decay_shift, decay_spike,
    rate_down, rate_up, rate_base, head_gain, w_out, xb, gain_b, ids, weights,
    e_gate, e_up, e_down, s_gate, s_up, s_down,
    out_a, out_b,
    v_xa, v_qkv, v_dd, v_rd, v_shift, v_spike, v_out, v_egu, v_ed, v_sgu, v_sd,
    tx, rx, rtx, rrx, X, Y, PR, Z, RA, RB, FA, FD, FB, FE, CA, CB,
    YA, PA, ZA, RAa, RBa, FAa, FDa, FBa, FEa, CAa, CBa,
    cmat, umat, mixed, atx, arx, ztx, zrx, btx, brx, sel_hi, sel_lo,
    lsem, tsem, rsem, ssend, srecv,
):
    z, x, y, c = (lax.axis_index(name) for name in ("z", "x", "y", "c"))
    yp, ym, cc = (y + 1) & 3, (y + 3) & 3, 1 - c
    used = [0]
    started = []

    local = {}

    def fetch(name, src, dst):
        copy = pltpu.make_async_copy(src, dst, lsem.at[len(local)])
        copy.start()
        local[name] = copy

    fetch("xa", xa, v_xa)
    fetch("wq", wq, v_qkv.at[:, 0:256])
    fetch("wk", wk, v_qkv.at[:, 256:512])
    fetch("wv", wv, v_qkv.at[:, 512:768])
    fetch("dd", decay_down, v_dd)
    fetch("rd", rate_down, v_rd)
    fetch("shift", decay_shift, v_shift)
    fetch("spike", decay_spike, v_spike)
    fetch("sg", s_gate, v_sgu.at[:, 0:128])
    fetch("su", s_up, v_sgu.at[:, 128:256])
    fetch("sd", s_down, v_sd)
    fetch("eg", e_gate, v_egu.at[:, :, 0:128])
    fetch("eu", e_up, v_egu.at[:, :, 128:256])
    fetch("ed", e_down, v_ed)
    fetch("out", w_out, v_out)

    def arrive(*names):
        for name in names:
            local[name].wait()

    barrier = pltpu.get_barrier_semaphore()

    def peer(place):
        return {"z": (z + DZ[place // 4]) & 7, "x": (x + place % 4) & 3}

    def source(place):
        return {"z": (z - DZ[place // 4]) & 7, "x": (x - place % 4) & 3}

    for place in range(1, 32):
        pl.semaphore_signal(barrier, inc=1, device_id=peer(place), device_id_type=MESH)
    for target in ({"y": yp}, {"y": ym}, {"c": cc}):
        pl.semaphore_signal(barrier, inc=1, device_id=target, device_id_type=MESH)

    def send(src, dst, target):
        n = used[0]
        used[0] += 1
        copy = pltpu.make_async_remote_copy(
            src_ref=src, dst_ref=dst, send_sem=ssend.at[n], recv_sem=srecv.at[n],
            device_id=target, device_id_type=MESH,
        )
        copy.start()
        started.append(copy)
        return copy

    normed_b = rms(xb[...], gain_b[...])
    mine = 32 * (2 * y + c)
    pick = ones_where(iota((256, 128), 0) == mine + (iota((256, 128), 1) & 31))
    own_ids = dot(ids[...].astype(F32), pick).astype(jnp.int32)
    expert = iota((128, 128), 0) >> 1
    first, second = own_ids[0:1] == expert, own_ids[1:2] == expert
    named = ones_where(first | second)
    lane, row = iota((128, 128), 1), iota((128, 128), 0)
    earlier = ones_where(((row >> 5) == (lane >> 5)) & (row < lane))
    count = dot(named, earlier)
    taken = (first | second) & (count == (row & 1).astype(F32))
    spread = ones_where((iota((32, 128), 1) & 31) == iota((32, 128), 0))
    w_tiled = dot_exact_right(weights[...], spread)
    slot_weight = jnp.where(taken, jnp.where(first, w_tiled[0:1], w_tiled[1:2]), 0.0)
    R, S = iota((512, 128), 0), iota((512, 128), 1)
    turn = R >> 6
    dz = jnp.where((turn & 1) == 1, (turn + 1) >> 1, (8 - (turn >> 1)) & 7)
    group = (((z + dz) & 7) << 2) + ((x + ((R >> 4) & 3)) & 3)
    place_of = ones_where(S == (group << 2) + (R & 3))
    own_quarter = ((R >> 2) & 3) == (S >> 5)
    chosen = jnp.where(own_quarter, dot(place_of, ones_where(taken)), 0.0)
    outgoing = dot(chosen, quarter_rows(normed_b)).astype(BF)
    tx[...] = outgoing.reshape(32, 16, 512)
    rx[0] = outgoing[0:16]
    X[4, 0, 0] = normed_b

    pl.semaphore_wait(barrier, 34)
    dispatched = []
    for place in range(1, 32):
        copy = pltpu.make_async_remote_copy(
            src_ref=tx.at[place], dst_ref=rx.at[place], send_sem=tsem.at[place],
            recv_sem=rsem.at[place], device_id=peer(place), device_id_type=MESH,
        )
        copy.start()
        dispatched.append(copy)

    gathers = {}

    def gather1(k):
        own = X.at[k, 0, 0]
        gathers[k] = [
            send(own, X.at[k, 0, 3], {"y": yp}),
            send(own, X.at[k, 0, 1], {"y": ym}),
            send(own, X.at[k, 1, 0], {"c": cc}),
        ]

    def gather2(k):
        held = gathers[k]
        held[0].wait_recv()
        left = X.at[k, 0, 3]
        held.append(send(left.at[:, 0:HALF], X.at[k, 0, 2, :, 0:HALF], {"y": yp}))
        held.append(send(left, X.at[k, 1, 3], {"c": cc}))
        held[1].wait_recv()
        right = X.at[k, 0, 1]
        held.append(send(right.at[:, HALF:], X.at[k, 0, 2, :, HALF:], {"y": ym}))
        held.append(send(right, X.at[k, 1, 1], {"c": cc}))

    def gather3(k):
        held = gathers[k]
        held[3].wait_recv()
        held[5].wait_recv()
        held.append(send(X.at[k, 0, 2], X.at[k, 1, 2], {"c": cc}))

    def gather4(k):
        held = gathers[k]
        for n in (2, 4, 6, 7):
            held[n].wait_recv()

    gather1(4)

    by_place = [jnp.where(own_quarter, dot(place_of, part), 0.0).astype(BF) for part in split(slot_weight)]
    sel_hi[...], sel_lo[...] = by_place

    def tile_row(a):
        return (((a >> 1) & 7) << 4) + ((a >> 5) << 2) + (((a >> 4) & 1) << 1) + (a & 1)

    def unpack_matrix():
        return ones_where(lane == tile_row(row))

    def pack_matrix():
        return ones_where(row == tile_row(lane))

    def unpack(k):
        for place in range(8 * k, 8 * k + 8):
            if place:
                dispatched[place - 1].wait_recv()
        tiles = rx[8 * k : 8 * k + 8].reshape(128, 512)
        stacked = dot(unpack_matrix(), tiles).astype(BF)
        X[k, 0, 0] = quarter_lanes(stacked, 32)

    def hidden_of(rows, gate_up):
        both = dot(rows, gate_up)
        gate = both[:, 0:128]
        return (gate * sigmoid(gate) * both[:, 128:256]).astype(BF)

    def experts(k):
        for j in range(2):
            rows = X[k, :, :, 16 * j : 16 * j + 16, :].reshape(128, 2048)
            hidden = hidden_of(rows, v_egu[j])
            Y[k, :, :, 16 * j : 16 * j + 16, :] = dot(hidden, v_ed[j]).astype(BF).reshape(2, 4, 16, 2048)

    def shared_expert():
        rows = X[4].reshape(256, 2048)
        hidden = hidden_of(rows, v_sgu[...])
        Y[4] = dot(hidden, v_sd[...]).astype(BF).reshape(2, 4, 32, 2048)

    sums = {}

    def refs_of(k):
        if k == "a":
            return YA, PA, ZA, RAa, RBa, FAa, FDa, FBa, FEa, CAa, CBa
        return tuple(ref.at[k] for ref in (Y, PR, Z, RA, RB, FA, FD, FB, FE, CA, CB))

    def sum1(k):
        refs = refs_of(k)
        sums[k] = [send(refs[0].at[1], refs[1], {"c": cc})]

    def sum2(k):
        part, pair, total, ra, rb, fa, fd, fb, fe, ca, cb = refs_of(k)
        held = sums[k]
        held[0].wait_recv()
        total[...] = (part[0].astype(F32) + pair[...].astype(F32)).astype(BF)
        held.append(send(total.at[2, :, 0:HALF], ra, {"y": yp}))
        held.append(send(total.at[2, :, HALF:], rb, {"y": ym}))
        held.append(send(total.at[1, :, HALF:], fe, {"y": yp}))
        held.append(send(total.at[3, :, 0:HALF], fd, {"y": ym}))

    def sum3(k):
        part, pair, total, ra, rb, fa, fd, fb, fe, ca, cb = refs_of(k)
        held = sums[k]
        held[1].wait_recv()
        ca[...] = (total[1, :, 0:HALF].astype(F32) + ra[...].astype(F32)).astype(BF)
        held.append(send(ca, fa, {"y": yp}))
        held[2].wait_recv()
        cb[...] = (total[3, :, HALF:].astype(F32) + rb[...].astype(F32)).astype(BF)
        held.append(send(cb, fb, {"y": ym}))

    def sum4(k):
        part, pair, total, ra, rb, fa, fd, fb, fe, ca, cb = refs_of(k)
        for n in (3, 4, 5, 6):
            sums[k][n].wait_recv()
        low = total[0, :, 0:HALF].astype(F32) + (fa[...].astype(F32) + fd[...].astype(F32))
        high = total[0, :, HALF:].astype(F32) + (fb[...].astype(F32) + fe[...].astype(F32))
        return jnp.concatenate([low, high], axis=1)

    returned = []

    def give_back(k):
        stacked = quarter_rows(sum4(k).astype(BF))
        packed = dot(pack_matrix(), stacked).astype(BF)
        rtx[8 * k : 8 * k + 8] = packed.reshape(8, 16, 512)
        for place in range(8 * k, 8 * k + 8):
            if place == 0:
                rrx[0] = packed[0:16]
                continue
            copy = pltpu.make_async_remote_copy(
                src_ref=rtx.at[place], dst_ref=rrx.at[place], send_sem=tsem.at[32 + place],
                recv_sem=rsem.at[32 + place], device_id=source(place), device_id_type=MESH,
            )
            copy.start()
            returned.append(copy)

    proj = {}

    def project():
        arrive("xa", "wq", "wk", "wv", "dd", "rd", "shift", "spike")
        normed = rms(v_xa[...], gain_a[...])
        qkv = dot(normed, v_qkv[...])
        last = ((1,), (1,))
        low = jnp.tanh(dot(normed, v_dd[...], last)).astype(BF)
        logits = decay_bias[...] + dot(low, decay_up[...]) + v_shift[...]
        log_decay = v_spike[...] - ROOT * sigmoid(logits)
        rate_low = dot(normed, v_rd[...], last).astype(BF)
        rate = sigmoid(rate_base[...] + dot(rate_low, rate_up[...]))
        q, k, v = qkv[:, 0:256], qkv[:, 256:512], qkv[:, 512:768]
        same = ones_where((iota((256, 256), 0) >> 6) == (iota((256, 256), 1) >> 6))
        unit = k * lax.rsqrt(dot_exact_right(k * k, same) + unit_eps)
        write = unit * rate
        block = (row >> 5) == (lane >> 5)
        cum = dot_exact_left(ones_where(block & (lane <= row)), log_decay)
        total = dot_exact_left(ones_where(block), log_decay)
        middle = 0.5 * total
        fade_in = jnp.exp(cum - middle)
        fade_out = jnp.exp(middle - cum)
        proj["qf"] = q * fade_in
        proj["ef"] = -unit * jnp.exp(cum - log_decay - middle)
        proj["wf"] = write * fade_out
        proj["kf"] = k * fade_out
        proj["v"] = v
        proj["em"] = jnp.exp(middle)
        proj["end"] = jnp.exp(total)

    def head(h):
        at = slice(HEAD * h, HEAD * h + HEAD)
        qf, ef, wf, kf, v, em, end = (proj[n][:, at] for n in ("qf", "ef", "wf", "kf", "v", "em", "end"))
        last = ((1,), (1,))
        block = (row >> 5) == (lane >> 5)
        strict, upto = block & (lane < row), block & (lane <= row)
        erase_write = jnp.where(strict, dot(ef, wf, last), 0.0)
        erase_key = jnp.where(strict, dot(ef, kf, last), 0.0)
        query_write = jnp.where(upto, dot(qf, wf, last), 0.0)
        query_key = jnp.where(upto, dot(qf, kf, last), 0.0)
        inverse = jnp.where(row == lane, 1.0, 0.0)
        for level in range(5):
            size = 1 << level
            corner = ((row >> (level + 1)) == (lane >> (level + 1))) & ((row & size) != 0) & ((lane & size) == 0)
            off = jnp.where(corner, erase_write, 0.0)
            if level == 0:
                inverse = inverse + off
            else:
                inverse = inverse + dot3(dot3(inverse, off), inverse)
        right = jnp.concatenate([ef * em, dot(erase_key, v)], axis=1)
        held = dot3(inverse, right)
        shown = dot(query_write, held) + jnp.concatenate([qf * em, dot(query_key, v)], axis=1)
        wide = (128, 256)
        mine_only = (iota(wide, 0) >> 5) == (iota(wide, 1) >> 6)
        ends_w = jnp.where(mine_only, jnp.concatenate([wf * em] * 4, axis=1), 0.0)
        ends_k = jnp.where(mine_only, jnp.concatenate([kf * em] * 4, axis=1), 0.0)
        ends = jnp.concatenate([ends_w, ends_k], axis=0)
        felt = jnp.concatenate([held, jnp.concatenate([jnp.zeros_like(v), v], axis=1)], axis=0)
        maps = dot(ends.T, felt)
        lane2, row2 = iota((HEAD, 128), 1), iota((HEAD, 128), 0)
        state = jnp.where(lane2 == row2, 1.0, 0.0)
        pieces = []
        for n in range(4):
            t = slice(SPAN * n, SPAN * n + SPAN)
            piece = dot3(shown[t, 0:HEAD], state)
            pieces.append(piece + jnp.where(iota((SPAN, 128), 1) >= HEAD, shown[t], 0.0))
            fade = jnp.concatenate([end[SPAN * n : SPAN * n + 1]] * 2, axis=1)
            step = maps[HEAD * n : HEAD * n + HEAD] + jnp.where(lane2 == row2, fade, 0.0)
            state = step if n == 0 else compose(step, state)
        umat[h] = jnp.concatenate(pieces, axis=0)
        atx[h] = state.astype(BF)

    scan = {}

    def scan1():
        arx[0] = atx[x]
        scan["x"] = [
            send(atx.at[(x + d) & 3], arx.at[d], {"x": (x + d) & 3}) for d in range(1, 4)
        ]

    def scan2():
        for copy in scan["x"]:
            copy.wait_recv()
        state = arx[x & 3].astype(F32)
        cmat[0] = state
        for n in range(1, 4):
            state = compose(arx[(x - n) & 3].astype(F32), state)
            cmat[n] = state
        ztx[...] = state.astype(BF)
        zrx[0] = ztx[...]
        scan["z"] = [send(ztx, zrx.at[d], {"z": (z + d) & 7}) for d in range(1, 8)]

    def scan3():
        for copy in scan["z"]:
            copy.wait_recv()
        lane2, row2 = iota((HEAD, 128), 1), iota((HEAD, 128), 0)
        state = jnp.where(lane2 == row2, 1.0, 0.0)
        for n in range(7):
            after = compose(zrx[(z - n) & 7].astype(F32), state)
            state = jnp.where(jnp.broadcast_to(n < z, after.shape), after, state)
        btx[0] = state.astype(BF)
        for n in range(1, 4):
            btx[n] = compose(cmat[n - 1], state).astype(BF)
        brx[0] = btx[x]
        scan["b"] = [
            send(btx.at[(x + d) & 3], brx.at[d], {"x": (x + d) & 3}) for d in range(1, 4)
        ]

    def finish_heads():
        for copy in scan["b"]:
            copy.wait_recv()
        outs = []
        for h in range(4):
            u = umat[h]
            outs.append((u + dot3(u[:, 0:HEAD], brx[(x - h) & 3].astype(F32)))[:, HEAD:])
        out = jnp.concatenate(outs, axis=1)
        same = ones_where((iota((256, 256), 0) >> 6) == (iota((256, 256), 1) >> 6))
        centered = out - dot_exact_right(out, same) * (1.0 / HEAD)
        var = dot_exact_right(centered * centered, same) * (1.0 / HEAD)
        mixed[...] = (centered * lax.rsqrt(var + group_eps) * head_gain[...].astype(F32)).astype(BF)

    def project_out():
        arrive("out")
        rows = jnp.concatenate(
            [
                mixed[pl.ds(pl.multiple_of(16 * (2 * ((y + r) & 3) + side), 16), 16), :]
                for side in (c, cc)
                for r in range(4)
            ],
            axis=0,
        )
        YA[...] = dot(rows, v_out[...]).astype(BF).reshape(2, 4, 16, 2048)

    project()
    gather2(4)
    unpack(0)
    gather1(0)
    head(0)
    gather3(4)
    unpack(1)
    gather1(1)
    head(1)
    gather2(0)
    unpack(2)
    gather1(2)
    gather4(4)
    arrive("sg", "su", "sd")
    shared_expert()
    sum1(4)
    head(2)
    gather3(0)
    gather2(1)
    unpack(3)
    gather1(3)
    sum2(4)
    head(3)
    scan1()
    gather2(2)
    gather3(1)
    gather4(0)
    arrive("eg", "eu", "ed")
    experts(0)
    sum1(0)
    sum3(4)
    scan2()
    gather2(3)
    gather3(2)
    gather4(1)
    experts(1)
    sum1(1)
    sum2(0)
    scan3()
    gather3(3)
    gather4(2)
    experts(2)
    sum1(2)
    sum2(1)
    sum3(0)
    finish_heads()
    gather4(3)
    experts(3)
    sum1(3)
    sum2(2)
    sum3(1)
    project_out()
    sum1("a")
    give_back(0)
    sum2(3)
    sum3(2)
    sum2("a")
    give_back(1)
    sum3(3)
    give_back(2)
    sum3("a")
    give_back(3)
    out_a[...] = sum4("a").astype(BF)
    total = sum4(4)
    routed = None
    for k in range(4):
        for place in range(8 * k, 8 * k + 8):
            if place:
                returned[place - 1].wait_recv()
        tiles = rrx[8 * k : 8 * k + 8].reshape(128, 512)
        at = slice(128 * k, 128 * k + 128)
        part = dot(sel_hi[at].T, tiles) + dot(sel_lo[at].T, tiles)
        routed = part if routed is None else routed + part
    out_b[...] = (quarter_lanes(routed, 32) + total).astype(BF)
    for copy in started + dispatched + returned:
        copy.wait_send()


SENDS = 110


def per_device(
    xa, gain_a, wq, wk, wv, decay_down, decay_up, decay_bias, decay_shift, decay_spike,
    rate_down, rate_up, rate_base, head_gain, w_out, xb, gain_b, ids, weights,
    e_gate, e_up, e_down, s_gate, s_up, s_down,
):
    here = pl.BlockSpec(memory_space=pltpu.VMEM)
    away = pl.BlockSpec(memory_space=pl.ANY)
    operands = [
        (xa, away), (gain_a[None], here), (wq, away), (wk, away), (wv, away),
        (decay_down.T, away), (decay_up, here), (decay_bias[None], here),
        (decay_shift, away), (decay_spike, away), (rate_down.T, away), (rate_up, here),
        (rate_base[None], here), (head_gain[None], here), (w_out, away), (xb, here),
        (gain_b[None], here), (ids.T, here), (weights.T, here), (e_gate, away), (e_up, away),
        (e_down, away), (s_gate, away), (s_up, away), (s_down, away),
    ]
    vm = pltpu.VMEM
    sums = lambda n: [
        vm((4, n, 2048), BF), vm((4, n, 2048), BF)] + [vm((n, HALF), BF)] * 8
    stacked = [vm((5,) + s.shape, BF) for s in sums(32)]
    scratch = [
        vm((128, 2048), BF), vm((2048, 768), BF), vm((64, 2048), BF), vm((64, 2048), BF),
        vm((128, 256), F32), vm((128, 256), F32), vm((256, 2048), BF), vm((2, 2048, 256), BF),
        vm((2, 128, 2048), BF), vm((2048, 256), BF), vm((128, 2048), BF),
        vm((32, 16, 512), BF), vm((32, 16, 512), BF), vm((32, 16, 512), BF), vm((32, 16, 512), BF),
        vm((5, 2, 4, 32, 2048), BF), vm((5, 2, 4, 32, 2048), BF),
        *stacked,
        vm((2, 4, 16, 2048), BF), *sums(16),
        vm((4, 64, 128), F32), vm((4, 128, 128), F32), vm((128, 256), BF),
        vm((4, 64, 128), BF), vm((4, 64, 128), BF), vm((64, 128), BF), vm((8, 64, 128), BF),
        vm((4, 64, 128), BF), vm((4, 64, 128), BF), vm((512, 128), BF), vm((512, 128), BF),
        pltpu.SemaphoreType.DMA((15,)), pltpu.SemaphoreType.DMA((64,)), pltpu.SemaphoreType.DMA((64,)),
        pltpu.SemaphoreType.DMA((SENDS,)), pltpu.SemaphoreType.DMA((SENDS,)),
    ]
    return pl.pallas_call(
        kernel,
        out_shape=(jax.ShapeDtypeStruct((16, 2048), BF), jax.ShapeDtypeStruct((32, 2048), BF)),
        in_specs=[spec for _, spec in operands],
        out_specs=(here, here),
        scratch_shapes=scratch,
        compiler_params=pltpu.CompilerParams(
            collective_id=0, has_side_effects=True, vmem_limit_bytes=60 * 1024 * 1024
        ),
    )(*[array for array, _ in operands])


def solution(mesh):
    split_mesh = Mesh(mesh.devices.reshape(8, 4, 4, 2), ("z", "x", "y", "c"))
    ep, tp = ("z", "x"), ("y", "c")
    both = ep + tp
    return jax.shard_map(
        per_device,
        mesh=split_mesh,
        in_specs=(
            P(ep, None), P(), P(None, tp), P(None, tp), P(None, tp), P(), P(None, tp), P(tp),
            P(ep, tp), P(ep, tp), P(), P(None, tp), P(tp), P(tp), P(tp, None), P(both, None),
            P(), P(ep, None), P(both, None), P(ep, None, tp), P(ep, None, tp), P(ep, tp, None),
            P(None, tp), P(None, tp), P(tp, None),
        ),
        out_specs=(P(both, None), P(both, None)),
        check_vma=False,
    )
```

```python
import jax
import jax.numpy as jnp
from jax import lax
from jax.experimental import pallas as pl
from jax.experimental.pallas import tpu as pltpu
from jax.sharding import Mesh
from jax.sharding import PartitionSpec as P

MESH = pl.DeviceIdType.MESH
BF, F32 = jnp.bfloat16, jnp.float32
norm_eps = 1e-06
group_eps = 0.00064
unit_eps = 1e-06
ROOT = 0.6065306597126334

HEADS = 4
HEAD = 64
SPAN = 32
ROWS = 128
TOK = 32
CHUNKS = 4
HALF = 1024
DZ = (7, 2, 6, 3, 5, 4, 0, 1)
OWN = 24
PLACES = [place for place in range(32) if place != OWN]
TABLE = sum(d << (3 * n) for n, d in enumerate(DZ))


def iota(shape, dim):
    return lax.broadcasted_iota(jnp.int32, shape, dim)


def dot(a, b, dims=((1,), (0,))):
    return lax.dot_general(a.astype(BF), b.astype(BF), (dims, ((), ())), preferred_element_type=F32)


def split(a):
    high = a.astype(BF)
    return high, (a - high.astype(F32)).astype(BF)


def dot3(a, b):
    ah, al = split(a)
    bh, bl = split(b)
    return dot(ah, bh) + (dot(ah, bl) + dot(al, bh))


def dot_exact_left(a, b):
    bh, rest = b.astype(BF), None
    rest = b - bh.astype(F32)
    bm = rest.astype(BF)
    bl = (rest - bm.astype(F32)).astype(BF)
    return dot(a, bh) + (dot(a, bm) + dot(a, bl))


def dot_exact_right(a, b):
    ah = a.astype(BF)
    rest = a - ah.astype(F32)
    am = rest.astype(BF)
    al = (rest - am.astype(F32)).astype(BF)
    return dot(ah, b) + (dot(am, b) + dot(al, b))


def sigmoid(u):
    e = jnp.exp(-jnp.abs(u))
    return jnp.where(u >= 0, 1.0, e) / (1.0 + e)


def rms(values, gain):
    values = values.astype(F32)
    scaled = values * lax.rsqrt(jnp.mean(values * values, axis=-1, keepdims=True) + norm_eps)
    return (scaled * gain.astype(F32)).astype(BF)


def ones_where(mask, kind=BF):
    return jnp.where(mask, 1.0, 0.0).astype(kind)


def row_of(ref):
    return ref[...].reshape(1, ref.shape[0])


def compose(later, earlier):
    lane = iota(later.shape, 1)
    return dot3(later[:, :HEAD], earlier) + jnp.where(lane >= HEAD, later, 0.0)


def quarter_rows(matrix):
    return jnp.concatenate([matrix[:, 512 * q : 512 * (q + 1)] for q in range(4)], axis=0)


def quarter_lanes(matrix, rows):
    return jnp.concatenate([matrix[rows * q : rows * (q + 1)] for q in range(4)], axis=1)


def kernel(
    xa, h_gain_a, wq, wk, wv, decay_down, h_decay_up, h_decay_bias, decay_shift, decay_spike,
    rate_down, h_rate_up, h_rate_base, h_head_gain, w_out, h_xb, h_gain_b, h_ids, h_weights,
    e_gate, e_up, e_down, s_gate, s_up, s_down,
    out_a, out_b,
    v_xa, v_qkv, v_dd, v_rd, v_shift, v_spike, v_out, v_egu, v_ed, v_sgu, v_sd,
    gain_a, decay_up, decay_bias, rate_up, rate_base, head_gain, xb, gain_b, ids, weights,
    tx, rx, rtx, rrx, X, Y, PR, Z, RA, RB, FA, FD, FB, FE, CA, CB,
    YA, PA, ZA, RAa, RBa, FAa, FDa, FBa, FEa, CAa, CBa,
    cmat, umat, mixed, atx, arx, ztx, zrx, btx, brx, sel_hi, sel_lo,
    lsem, ssend, srecv,
):
    z, x, y, c = (lax.axis_index(name) for name in ("z", "x", "y", "c"))
    yp, ym, cc = (y + 1) & 3, (y + 3) & 3, 1 - c

    barrier = pltpu.get_barrier_semaphore()

    def peer(place):
        return {"z": (z + DZ[place // 4]) & 7, "x": (x + place % 4) & 3}

    def source(place):
        return {"z": (z - DZ[place // 4]) & 7, "x": (x - place % 4) & 3}

    for place in PLACES:
        pl.semaphore_signal(barrier, inc=1, device_id=peer(place), device_id_type=MESH)
    for target in ({"y": yp}, {"y": ym}, {"c": cc}):
        pl.semaphore_signal(barrier, inc=1, device_id=target, device_id_type=MESH)

    local = {}

    def fetch(name, src, dst):
        copy = pltpu.make_async_copy(src, dst, lsem.at[len(local)])
        copy.start()
        local[name] = copy

    fetch("xb", h_xb, xb)
    fetch("gain_b", h_gain_b, gain_b)
    fetch("ids", h_ids, ids)
    fetch("weights", h_weights, weights)
    fetch("xa", xa, v_xa)
    fetch("gain_a", h_gain_a, gain_a)
    fetch("decay_up", h_decay_up, decay_up)
    fetch("decay_bias", h_decay_bias, decay_bias)
    fetch("rate_up", h_rate_up, rate_up)
    fetch("rate_base", h_rate_base, rate_base)
    fetch("head_gain", h_head_gain, head_gain)
    fetch("wq", wq, v_qkv.at[:, 0:256])
    fetch("wk", wk, v_qkv.at[:, 256:512])
    fetch("wv", wv, v_qkv.at[:, 512:768])
    fetch("dd", decay_down, v_dd)
    fetch("rd", rate_down, v_rd)
    fetch("shift", decay_shift, v_shift)
    fetch("spike", decay_spike, v_spike)
    fetch("sg", s_gate, v_sgu.at[:, 0:128])
    fetch("su", s_up, v_sgu.at[:, 128:256])
    fetch("sd", s_down, v_sd)
    fetch("eg", e_gate, v_egu.at[:, :, 0:128])
    fetch("eu", e_up, v_egu.at[:, :, 128:256])
    fetch("ed", e_down, v_ed)
    fetch("out", w_out, v_out)

    def arrive(*names):
        for name in names:
            local[name].wait()

    send_names, recv_names = {}, {}

    def send(src, dst, target, leaving, landing):
        pltpu.make_async_remote_copy(
            src_ref=src, dst_ref=dst,
            send_sem=ssend.at[send_names.setdefault(leaving, len(send_names))],
            recv_sem=srecv.at[recv_names.setdefault(landing, len(recv_names))],
            device_id=target, device_id_type=MESH,
        ).start()

    def take(ref, landing):
        pltpu.make_async_copy(ref, ref, srecv.at[recv_names[landing]]).wait()

    def sent(ref, leaving):
        pltpu.make_async_copy(ref, ref, ssend.at[send_names[leaving]]).wait()

    arrive("xb", "gain_b", "ids", "weights")
    normed_b = rms(xb[...], row_of(gain_b))
    mine = 32 * (2 * y + c)
    pick = ones_where(iota((256, 128), 0) == mine + (iota((256, 128), 1) & 31))
    own_ids = dot(ids[...].astype(F32), pick).astype(jnp.int32)
    expert = iota((128, 128), 0) >> 1
    first, second = own_ids[0:1] == expert, own_ids[1:2] == expert
    named = ones_where(first | second)
    lane, row = iota((128, 128), 1), iota((128, 128), 0)
    earlier = ones_where(((row >> 5) == (lane >> 5)) & (row < lane))
    count = dot(named, earlier)
    taken = (first | second) & (count == (row & 1).astype(F32))
    spread = ones_where((iota((32, 128), 1) & 31) == iota((32, 128), 0))
    w_tiled = dot_exact_right(weights[...], spread)
    slot_weight = jnp.where(taken, jnp.where(first, w_tiled[0:1], w_tiled[1:2]), 0.0)
    R, S = iota((512, 128), 0), iota((512, 128), 1)
    dz = lax.shift_right_logical(jnp.full_like(R, TABLE), 3 * (R >> 6)) & 7
    group = (((z + dz) & 7) << 2) + ((x + ((R >> 4) & 3)) & 3)
    place_of = ones_where(S == (group << 2) + (R & 3))
    own_quarter = ((R >> 2) & 3) == (S >> 5)
    chosen = jnp.where(own_quarter, dot(place_of, ones_where(taken)), 0.0)
    outgoing = dot(chosen, quarter_rows(normed_b)).astype(BF)
    tx[...] = outgoing.reshape(32, 16, 512)
    rx[OWN] = outgoing[16 * OWN : 16 * OWN + 16]
    X[4, 0] = normed_b

    pl.semaphore_wait(barrier, 34)
    for place in PLACES:
        send(tx.at[place], rx.at[place], peer(place), "d", ("d", place // 8))

    def tiles_of(ref, k):
        return ref.at[OWN + 1 : 32] if k == OWN // 8 else ref.at[8 * k : 8 * k + 8]

    def gather1(k):
        own = X.at[k, 0]
        send(own, X.at[k, 3], {"y": yp}, ("g", k), ("gl", k))
        send(own, X.at[k, 1], {"y": ym}, ("g", k), ("gr", k))
        send(own, X.at[k, 4], {"c": cc}, ("g", k), ("gc", k))

    def gather2(k):
        left, right = X.at[k, 3], X.at[k, 1]
        take(left, ("gl", k))
        send(left.at[:, 0:HALF], X.at[k, 2, :, 0:HALF], {"y": yp}, ("g", k), ("gh", k))
        send(left, X.at[k, 7], {"c": cc}, ("g", k), ("gc", k))
        take(right, ("gr", k))
        send(right.at[:, HALF:], X.at[k, 2, :, HALF:], {"y": ym}, ("g", k), ("gh", k))
        send(right, X.at[k, 5], {"c": cc}, ("g", k), ("gc", k))

    def gather3(k):
        take(X.at[k, 2], ("gh", k))
        send(X.at[k, 2], X.at[k, 6], {"c": cc}, ("g", k), ("gc", k))

    def gather4(k):
        take(X.at[k, 4:8], ("gc", k))

    gather1(4)

    by_place = [jnp.where(own_quarter, dot(place_of, part), 0.0).astype(BF) for part in split(slot_weight)]
    sel_hi[...], sel_lo[...] = by_place

    def tile_row(a):
        return (((a >> 1) & 7) << 4) + ((a >> 5) << 2) + (((a >> 4) & 1) << 1) + (a & 1)

    def unpack_matrix():
        return ones_where(lane == tile_row(row))

    def pack_matrix():
        return ones_where(row == tile_row(lane))

    def unpack(k):
        take(tiles_of(rx, k), ("d", k))
        tiles = rx[8 * k : 8 * k + 8].reshape(128, 512)
        stacked = dot(unpack_matrix(), tiles).astype(BF)
        X[k, 0] = quarter_lanes(stacked, 32)

    def hidden_of(rows, gate_up):
        both = dot(rows, gate_up)
        gate = both[:, 0:128]
        return (gate * sigmoid(gate) * both[:, 128:256]).astype(BF)

    def experts(k):
        for j in range(2):
            rows = X[k, :, 16 * j : 16 * j + 16, :].reshape(128, 2048)
            hidden = hidden_of(rows, v_egu[j])
            Y[k, :, 16 * j : 16 * j + 16, :] = dot(hidden, v_ed[j]).astype(BF).reshape(8, 16, 2048)

    def shared_expert():
        rows = X[4].reshape(256, 2048)
        hidden = hidden_of(rows, v_sgu[...])
        Y[4] = dot(hidden, v_sd[...]).astype(BF).reshape(8, 32, 2048)

    def refs_of(k):
        if k == "a":
            return YA, PA, ZA, RAa, RBa, FAa, FDa, FBa, FEa, CAa, CBa
        return tuple(ref.at[k] for ref in (Y, PR, Z, RA, RB, FA, FD, FB, FE, CA, CB))

    def sum1(k):
        refs = refs_of(k)
        send(refs[0].at[4:8], refs[1], {"c": cc}, ("s", k), ("sp", k))

    def sum2(k):
        part, pair, total, ra, rb, fa, fd, fb, fe, ca, cb = refs_of(k)
        take(pair, ("sp", k))
        total[...] = (part[0:4].astype(F32) + pair[...].astype(F32)).astype(BF)
        send(total.at[2, :, 0:HALF], ra, {"y": yp}, ("s", k), ("sa", k))
        send(total.at[2, :, HALF:], rb, {"y": ym}, ("s", k), ("sb", k))
        send(total.at[1, :, HALF:], fe, {"y": yp}, ("s", k), ("sf", k))
        send(total.at[3, :, 0:HALF], fd, {"y": ym}, ("s", k), ("sf", k))

    def sum3(k):
        part, pair, total, ra, rb, fa, fd, fb, fe, ca, cb = refs_of(k)
        take(ra, ("sa", k))
        ca[...] = (total[1, :, 0:HALF].astype(F32) + ra[...].astype(F32)).astype(BF)
        send(ca, fa, {"y": yp}, ("s", k), ("sf", k))
        take(rb, ("sb", k))
        cb[...] = (total[3, :, HALF:].astype(F32) + rb[...].astype(F32)).astype(BF)
        send(cb, fb, {"y": ym}, ("s", k), ("sf", k))

    def sum4(k):
        part, pair, total, ra, rb, fa, fd, fb, fe, ca, cb = refs_of(k)
        take(total.at[0:2], ("sf", k))
        low = total[0, :, 0:HALF].astype(F32) + (fa[...].astype(F32) + fd[...].astype(F32))
        high = total[0, :, HALF:].astype(F32) + (fb[...].astype(F32) + fe[...].astype(F32))
        return jnp.concatenate([low, high], axis=1)

    def give_back(k):
        stacked = quarter_rows(sum4(k).astype(BF))
        packed = dot(pack_matrix(), stacked).astype(BF)
        rtx[8 * k : 8 * k + 8] = packed.reshape(8, 16, 512)
        for place in range(8 * k, 8 * k + 8):
            if place == OWN:
                rrx[OWN] = packed[0:16]
            else:
                send(rtx.at[place], rrx.at[place], source(place), "r", ("r", k))

    proj = {}

    def project():
        arrive("xa", "gain_a", "wq", "wk", "wv", "dd", "rd", "shift", "spike")
        arrive("decay_up", "decay_bias", "rate_up", "rate_base", "head_gain")
        normed = rms(v_xa[...], row_of(gain_a))
        qkv = dot(normed, v_qkv[...])
        last = ((1,), (1,))
        low = jnp.tanh(dot(normed, v_dd[...], last)).astype(BF)
        logits = decay_bias[...] + dot(low, decay_up[...]) + v_shift[...]
        log_decay = v_spike[...] - ROOT * sigmoid(logits)
        rate_low = dot(normed, v_rd[...], last).astype(BF)
        rate = sigmoid(rate_base[...] + dot(rate_low, rate_up[...]))
        q, k, v = qkv[:, 0:256], qkv[:, 256:512], qkv[:, 512:768]
        same = ones_where((iota((256, 256), 0) >> 6) == (iota((256, 256), 1) >> 6))
        unit = k * lax.rsqrt(dot_exact_right(k * k, same) + unit_eps)
        write = unit * rate
        block = (row >> 5) == (lane >> 5)
        cum = dot_exact_left(ones_where(block & (lane <= row)), log_decay)
        total = dot_exact_left(ones_where(block), log_decay)
        middle = 0.5 * total
        fade_in = jnp.exp(cum - middle)
        fade_out = jnp.exp(middle - cum)
        proj["qf"] = q * fade_in
        proj["ef"] = -unit * jnp.exp(cum - log_decay - middle)
        proj["wf"] = write * fade_out
        proj["kf"] = k * fade_out
        proj["v"] = v
        proj["em"] = jnp.exp(middle)
        proj["end"] = jnp.exp(total)

    def head(h):
        at = slice(HEAD * h, HEAD * h + HEAD)
        qf, ef, wf, kf, v, em, end = (proj[n][:, at] for n in ("qf", "ef", "wf", "kf", "v", "em", "end"))
        last = ((1,), (1,))
        block = (row >> 5) == (lane >> 5)
        strict, upto = block & (lane < row), block & (lane <= row)
        erase_write = jnp.where(strict, dot(ef, wf, last), 0.0)
        erase_key = jnp.where(strict, dot(ef, kf, last), 0.0)
        query_write = jnp.where(upto, dot(qf, wf, last), 0.0)
        query_key = jnp.where(upto, dot(qf, kf, last), 0.0)
        yield
        inverse = jnp.where(row == lane, 1.0, 0.0)
        for level in range(5):
            size = 1 << level
            corner = ((row >> (level + 1)) == (lane >> (level + 1))) & ((row & size) != 0) & ((lane & size) == 0)
            off = jnp.where(corner, erase_write, 0.0)
            if level == 0:
                inverse = inverse + off
            else:
                inverse = inverse + dot3(dot3(inverse, off), inverse)
                yield
        right = jnp.concatenate([ef * em, dot(erase_key, v)], axis=1)
        held = dot3(inverse, right)
        shown = dot(query_write, held) + jnp.concatenate([qf * em, dot(query_key, v)], axis=1)
        yield
        wide = (128, 256)
        mine_only = (iota(wide, 0) >> 5) == (iota(wide, 1) >> 6)
        ends_w = jnp.where(mine_only, jnp.concatenate([wf * em] * 4, axis=1), 0.0)
        ends_k = jnp.where(mine_only, jnp.concatenate([kf * em] * 4, axis=1), 0.0)
        ends = jnp.concatenate([ends_w, ends_k], axis=0)
        felt = jnp.concatenate([held, jnp.concatenate([jnp.zeros_like(v), v], axis=1)], axis=0)
        maps = dot(ends.T, felt)
        yield
        lane2, row2 = iota((HEAD, 128), 1), iota((HEAD, 128), 0)
        state = jnp.where(lane2 == row2, 1.0, 0.0)
        pieces = []
        for n in range(4):
            t = slice(SPAN * n, SPAN * n + SPAN)
            piece = dot3(shown[t, 0:HEAD], state)
            pieces.append(piece + jnp.where(iota((SPAN, 128), 1) >= HEAD, shown[t], 0.0))
            fade = jnp.concatenate([end[SPAN * n : SPAN * n + 1]] * 2, axis=1)
            step = maps[HEAD * n : HEAD * n + HEAD] + jnp.where(lane2 == row2, fade, 0.0)
            state = step if n == 0 else compose(step, state)
            yield
        umat[h] = jnp.concatenate(pieces, axis=0)
        atx[h] = state.astype(BF)
        yield

    walks = []

    def heads(steps):
        if not walks:
            walks.extend(head(h) for h in range(HEADS))
        for _ in range(steps):
            for walk in walks:
                next(walk)

    def scan1():
        arx[0] = atx[x]
        for d in range(1, 4):
            send(atx.at[(x + d) & 3], arx.at[d], {"x": (x + d) & 3}, "x", "x")

    def scan2():
        take(arx.at[1:4], "x")
        state = arx[x & 3].astype(F32)
        cmat[0] = state
        for n in range(1, 4):
            state = compose(arx[(x - n) & 3].astype(F32), state)
            cmat[n] = state
        ztx[...] = state.astype(BF)
        zrx[0] = ztx[...]
        for d in range(1, 8):
            send(ztx, zrx.at[d], {"z": (z + d) & 7}, "z", "z")

    def scan3():
        take(zrx.at[1:8], "z")
        lane2, row2 = iota((HEAD, 128), 1), iota((HEAD, 128), 0)
        state = jnp.where(lane2 == row2, 1.0, 0.0)
        for n in range(7):
            after = compose(zrx[(z - n) & 7].astype(F32), state)
            state = jnp.where(jnp.broadcast_to(n < z, after.shape), after, state)
        btx[0] = state.astype(BF)
        for n in range(1, 4):
            btx[n] = compose(cmat[n - 1], state).astype(BF)
        brx[0] = btx[x]
        for d in range(1, 4):
            send(btx.at[(x + d) & 3], brx.at[d], {"x": (x + d) & 3}, "b", "b")

    def finish_heads():
        take(brx.at[1:4], "b")
        outs = []
        for h in range(4):
            u = umat[h]
            outs.append((u + dot3(u[:, 0:HEAD], brx[(x - h) & 3].astype(F32)))[:, HEAD:])
        out = jnp.concatenate(outs, axis=1)
        same = ones_where((iota((256, 256), 0) >> 6) == (iota((256, 256), 1) >> 6))
        centered = out - dot_exact_right(out, same) * (1.0 / HEAD)
        var = dot_exact_right(centered * centered, same) * (1.0 / HEAD)
        mixed[...] = (centered * lax.rsqrt(var + group_eps) * row_of(head_gain).astype(F32)).astype(BF)

    def project_out():
        arrive("out")
        rows = jnp.concatenate(
            [
                mixed[pl.ds(pl.multiple_of(16 * (2 * ((y + r) & 3) + side), 16), 16), :]
                for side in (c, cc)
                for r in range(4)
            ],
            axis=0,
        )
        YA[...] = dot(rows, v_out[...]).astype(BF).reshape(8, 16, 2048)

    project()
    heads(2)
    gather2(4)
    unpack(0)
    gather1(0)
    heads(2)
    unpack(1)
    gather1(1)
    heads(1)
    gather2(0)
    heads(1)
    unpack(2)
    gather1(2)
    gather2(1)
    heads(1)
    unpack(3)
    gather1(3)
    heads(5)
    scan1()
    gather3(0)
    gather4(0)
    arrive("eg", "eu", "ed")
    experts(0)
    sum1(0)
    gather2(2)
    gather3(1)
    sum2(0)
    gather3(4)
    gather2(3)
    gather4(1)
    experts(1)
    sum1(1)
    scan2()
    gather3(2)
    sum2(1)
    sum3(0)
    gather4(2)
    experts(2)
    sum1(2)
    gather3(3)
    sum2(2)
    sum3(1)
    gather4(3)
    experts(3)
    sum1(3)
    gather4(4)
    arrive("sg", "su", "sd")
    shared_expert()
    sum1(4)
    give_back(0)
    scan3()
    sum2(3)
    sum3(2)
    give_back(1)
    finish_heads()
    project_out()
    sum1("a")
    sum2(4)
    sum3(3)
    give_back(2)
    sum2("a")
    sum3(4)
    give_back(3)
    sum3("a")
    total = sum4(4)
    out_a[...] = sum4("a").astype(BF)
    routed = None
    for k in range(CHUNKS):
        take(tiles_of(rrx, k), ("r", k))
        tiles = rrx[8 * k : 8 * k + 8].reshape(128, 512)
        at = slice(128 * k, 128 * k + 128)
        part = dot(sel_hi[at].T, tiles) + dot(sel_lo[at].T, tiles)
        routed = part if routed is None else routed + part
    out_b[...] = (quarter_lanes(routed, 32) + total).astype(BF)
    for k in range(5):
        sent(X.at[k, 0:7], ("g", k))
        sent(Y.at[k, 0:7], ("s", k))
    sent(YA.at[0:7], ("s", "a"))
    sent(atx.at[0:3], "x")
    sent(zrx.at[0:7], "z")
    sent(btx.at[0:3], "b")
    sent(tx.at[0:31], "d")
    sent(rtx.at[0:31], "r")
    assert (len(send_names), len(recv_names)) == (LEAVING, LANDING)


LEAVING, LANDING = 16, 55


def per_device(
    xa, gain_a, wq, wk, wv, decay_down, decay_up, decay_bias, decay_shift, decay_spike,
    rate_down, rate_up, rate_base, head_gain, w_out, xb, gain_b, ids, weights,
    e_gate, e_up, e_down, s_gate, s_up, s_down,
):
    here = pl.BlockSpec(memory_space=pltpu.VMEM)
    away = pl.BlockSpec(memory_space=pl.ANY)
    operands = [
        (xa, away), (gain_a, away), (wq, away), (wk, away), (wv, away),
        (decay_down.T, away), (decay_up, away), (decay_bias[None], away),
        (decay_shift, away), (decay_spike, away), (rate_down.T, away), (rate_up, away),
        (rate_base[None], away), (head_gain, away), (w_out, away), (xb, away),
        (gain_b, away), (ids.T, away), (weights.T, away), (e_gate, away), (e_up, away),
        (e_down, away), (s_gate, away), (s_up, away), (s_down, away),
    ]
    vm = pltpu.VMEM
    sums = lambda n: [
        vm((4, n, 2048), BF), vm((4, n, 2048), BF)] + [vm((n, HALF), BF)] * 8
    stacked = [vm((5,) + s.shape, BF) for s in sums(32)]
    scratch = [
        vm((128, 2048), BF), vm((2048, 768), BF), vm((64, 2048), BF), vm((64, 2048), BF),
        vm((128, 256), F32), vm((128, 256), F32), vm((256, 2048), BF), vm((2, 2048, 256), BF),
        vm((2, 128, 2048), BF), vm((2048, 256), BF), vm((128, 2048), BF),
        vm((2048,), BF), vm((64, 256), BF), vm((1, 256), F32), vm((64, 256), BF), vm((1, 256), F32),
        vm((256,), BF), vm((32, 2048), BF), vm((2048,), BF), vm((2, 256), jnp.int32), vm((2, 32), F32),
        vm((32, 16, 512), BF), vm((32, 16, 512), BF), vm((32, 16, 512), BF), vm((32, 16, 512), BF),
        vm((5, 8, 32, 2048), BF), vm((5, 8, 32, 2048), BF),
        *stacked,
        vm((8, 16, 2048), BF), *sums(16),
        vm((4, 64, 128), F32), vm((4, 128, 128), F32), vm((128, 256), BF),
        vm((4, 64, 128), BF), vm((4, 64, 128), BF), vm((64, 128), BF), vm((8, 64, 128), BF),
        vm((4, 64, 128), BF), vm((4, 64, 128), BF), vm((512, 128), BF), vm((512, 128), BF),
        pltpu.SemaphoreType.DMA((25,)), pltpu.SemaphoreType.DMA((LEAVING,)),
        pltpu.SemaphoreType.DMA((LANDING,)),
    ]
    return pl.pallas_call(
        kernel,
        out_shape=(vm((16, 2048), BF), vm((32, 2048), BF)),
        in_specs=[spec for _, spec in operands],
        out_specs=(here, here),
        scratch_shapes=scratch,
        compiler_params=pltpu.CompilerParams(
            collective_id=0, has_side_effects=True, vmem_limit_bytes=60 * 1024 * 1024
        ),
    )(*[array for array, _ in operands])


def solution(mesh):
    split_mesh = Mesh(mesh.devices.reshape(8, 4, 4, 2), ("z", "x", "y", "c"))
    ep, tp = ("z", "x"), ("y", "c")
    both = ep + tp
    return jax.shard_map(
        per_device,
        mesh=split_mesh,
        in_specs=(
            P(ep, None), P(), P(None, tp), P(None, tp), P(None, tp), P(), P(None, tp), P(tp),
            P(ep, tp), P(ep, tp), P(), P(None, tp), P(tp), P(tp), P(tp, None), P(both, None),
            P(), P(ep, None), P(both, None), P(ep, None, tp), P(ep, None, tp), P(ep, tp, None),
            P(None, tp), P(None, tp), P(tp, None),
        ),
        out_specs=(P(both, None), P(both, None)),
        check_vma=False,
    )
```

```python
import jax
import jax.numpy as jnp
from jax import lax
from jax.experimental import pallas as pl
from jax.experimental.pallas import tpu as pltpu
from jax.sharding import Mesh
from jax.sharding import PartitionSpec as P

MESH = pl.DeviceIdType.MESH
BF, F32 = jnp.bfloat16, jnp.float32
norm_eps = 1e-06
group_eps = 0.00064
unit_eps = 1e-06
ROOT = 0.6065306597126334

HEADS = 4
HEAD = 64
SPAN = 32
ROWS = 128
TOK = 32
CHUNKS = 4
HALF = 1024
DZ = (7, 2, 6, 3, 5, 4, 0, 1)
OWN = 24
PLACES = [place for place in range(32) if place != OWN]
TABLE = sum(d << (3 * n) for n, d in enumerate(DZ))


def iota(shape, dim):
    return lax.broadcasted_iota(jnp.int32, shape, dim)


def dot(a, b, dims=((1,), (0,))):
    return lax.dot_general(a.astype(BF), b.astype(BF), (dims, ((), ())), preferred_element_type=F32)


def split(a):
    high = a.astype(BF)
    return high, (a - high.astype(F32)).astype(BF)


def dot3(a, b):
    ah, al = split(a)
    bh, bl = split(b)
    return dot(ah, bh) + (dot(ah, bl) + dot(al, bh))


def dot_exact_left(a, b):
    bh, rest = b.astype(BF), None
    rest = b - bh.astype(F32)
    bm = rest.astype(BF)
    bl = (rest - bm.astype(F32)).astype(BF)
    return dot(a, bh) + (dot(a, bm) + dot(a, bl))


def dot_exact_right(a, b):
    ah = a.astype(BF)
    rest = a - ah.astype(F32)
    am = rest.astype(BF)
    al = (rest - am.astype(F32)).astype(BF)
    return dot(ah, b) + (dot(am, b) + dot(al, b))


def sigmoid(u):
    e = jnp.exp(-jnp.abs(u))
    return jnp.where(u >= 0, 1.0, e) / (1.0 + e)


def rms(values, gain):
    values = values.astype(F32)
    scaled = values * lax.rsqrt(jnp.mean(values * values, axis=-1, keepdims=True) + norm_eps)
    return (scaled * gain.astype(F32)).astype(BF)


def ones_where(mask, kind=BF):
    return jnp.where(mask, 1.0, 0.0).astype(kind)


def row_of(ref):
    return ref[...].reshape(1, ref.shape[0])


def compose(later, earlier):
    lane = iota(later.shape, 1)
    return dot3(later[:, :HEAD], earlier) + jnp.where(lane >= HEAD, later, 0.0)


def quarter_rows(matrix):
    return jnp.concatenate([matrix[:, 512 * q : 512 * (q + 1)] for q in range(4)], axis=0)


def quarter_lanes(matrix, rows):
    return jnp.concatenate([matrix[rows * q : rows * (q + 1)] for q in range(4)], axis=1)


def kernel(
    xa, h_gain_a, wq, wk, wv, decay_down, h_decay_up, h_decay_bias, decay_shift, decay_spike,
    rate_down, h_rate_up, h_rate_base, h_head_gain, w_out, h_xb, h_gain_b, h_ids, h_weights,
    e_gate, e_up, e_down, s_gate, s_up, s_down,
    out_a, out_b,
    v_xa, v_qkv, v_dd, v_rd, v_shift, v_spike, v_out, v_egu, v_ed, v_sgu, v_sd,
    gain_a, decay_up, decay_bias, rate_up, rate_base, head_gain, xb, gain_b, ids, weights,
    tx, rx, rtx, rrx, X, Y, PR, Z, RA, RB, FA, FD, FB, FE, CA, CB,
    YA, PA, ZA, RAa, RBa, FAa, FDa, FBa, FEa, CAa, CBa,
    cmat, umat, mixed, atx, arx, ztx, zrx, btx, brx, sel_hi, sel_lo,
    lsem, ssend, srecv,
):
    z, x, y, c = (lax.axis_index(name) for name in ("z", "x", "y", "c"))
    yp, ym, cc = (y + 1) & 3, (y + 3) & 3, 1 - c

    barrier = pltpu.get_barrier_semaphore()

    def peer(place):
        return {"z": (z + DZ[place // 4]) & 7, "x": (x + place % 4) & 3}

    def source(place):
        return {"z": (z - DZ[place // 4]) & 7, "x": (x - place % 4) & 3}

    for place in PLACES:
        pl.semaphore_signal(barrier, inc=1, device_id=peer(place), device_id_type=MESH)
    for target in ({"y": yp}, {"y": ym}, {"c": cc}):
        pl.semaphore_signal(barrier, inc=1, device_id=target, device_id_type=MESH)

    local = {}

    def fetch(name, src, dst):
        copy = pltpu.make_async_copy(src, dst, lsem.at[len(local)])
        copy.start()
        local[name] = copy

    fetch("xb", h_xb, xb)
    fetch("gain_b", h_gain_b, gain_b)
    fetch("ids", h_ids, ids)
    fetch("weights", h_weights, weights)
    fetch("xa", xa, v_xa)
    fetch("gain_a", h_gain_a, gain_a)
    fetch("decay_up", h_decay_up, decay_up)
    fetch("decay_bias", h_decay_bias, decay_bias)
    fetch("rate_up", h_rate_up, rate_up)
    fetch("rate_base", h_rate_base, rate_base)
    fetch("head_gain", h_head_gain, head_gain)
    fetch("wq", wq, v_qkv.at[:, 0:256])
    fetch("wk", wk, v_qkv.at[:, 256:512])
    fetch("wv", wv, v_qkv.at[:, 512:768])
    fetch("dd", decay_down, v_dd)
    fetch("rd", rate_down, v_rd)
    fetch("shift", decay_shift, v_shift)
    fetch("spike", decay_spike, v_spike)
    fetch("sg", s_gate, v_sgu.at[:, 0:128])
    fetch("su", s_up, v_sgu.at[:, 128:256])
    fetch("sd", s_down, v_sd)
    fetch("eg", e_gate, v_egu.at[:, :, 0:128])
    fetch("eu", e_up, v_egu.at[:, :, 128:256])
    fetch("ed", e_down, v_ed)
    fetch("out", w_out, v_out)

    def arrive(*names):
        for name in names:
            local[name].wait()

    send_names, recv_names = {}, {}

    def send(src, dst, target, leaving, landing):
        pltpu.make_async_remote_copy(
            src_ref=src, dst_ref=dst,
            send_sem=ssend.at[send_names.setdefault(leaving, len(send_names))],
            recv_sem=srecv.at[recv_names.setdefault(landing, len(recv_names))],
            device_id=target, device_id_type=MESH,
        ).start()

    def take(ref, landing):
        pltpu.make_async_copy(ref, ref, srecv.at[recv_names[landing]]).wait()

    def sent(ref, leaving):
        pltpu.make_async_copy(ref, ref, ssend.at[send_names[leaving]]).wait()

    arrive("xb", "gain_b", "ids", "weights")
    normed_b = rms(xb[...], row_of(gain_b))
    mine = 32 * (2 * y + c)
    pick = ones_where(iota((256, 128), 0) == mine + (iota((256, 128), 1) & 31))
    own_ids = dot(ids[...].astype(F32), pick).astype(jnp.int32)
    expert = iota((128, 128), 0) >> 1
    first, second = own_ids[0:1] == expert, own_ids[1:2] == expert
    named = ones_where(first | second)
    lane, row = iota((128, 128), 1), iota((128, 128), 0)
    earlier = ones_where(((row >> 5) == (lane >> 5)) & (row < lane))
    count = dot(named, earlier)
    taken = (first | second) & (count == (row & 1).astype(F32))
    spread = ones_where((iota((32, 128), 1) & 31) == iota((32, 128), 0))
    w_tiled = dot_exact_right(weights[...], spread)
    slot_weight = jnp.where(taken, jnp.where(first, w_tiled[0:1], w_tiled[1:2]), 0.0)
    R, S = iota((512, 128), 0), iota((512, 128), 1)
    dz = lax.shift_right_logical(jnp.full_like(R, TABLE), 3 * (R >> 6)) & 7
    group = (((z + dz) & 7) << 2) + ((x + ((R >> 4) & 3)) & 3)
    place_of = ones_where(S == (group << 2) + (R & 3))
    own_quarter = ((R >> 2) & 3) == (S >> 5)
    chosen = jnp.where(own_quarter, dot(place_of, ones_where(taken)), 0.0)
    outgoing = dot(chosen, quarter_rows(normed_b)).astype(BF)
    tx[...] = outgoing.reshape(32, 16, 512)
    rx[OWN] = outgoing[16 * OWN : 16 * OWN + 16]
    X[4, 0] = normed_b

    pl.semaphore_wait(barrier, 34)
    for place in PLACES:
        send(tx.at[place], rx.at[place], peer(place), "d", ("d", place // 8))

    def tiles_of(ref, k):
        return ref.at[OWN + 1 : 32] if k == OWN // 8 else ref.at[8 * k : 8 * k + 8]

    def gather1(k):
        own = X.at[k, 0]
        send(own, X.at[k, 3], {"y": yp}, ("g", k), ("gl", k))
        send(own, X.at[k, 1], {"y": ym}, ("g", k), ("gr", k))
        send(own, X.at[k, 4], {"c": cc}, ("g", k), ("gc", k))

    def gather2(k):
        left, right = X.at[k, 3], X.at[k, 1]
        take(left, ("gl", k))
        send(left.at[:, 0:HALF], X.at[k, 2, :, 0:HALF], {"y": yp}, ("g", k), ("gh", k))
        send(left, X.at[k, 7], {"c": cc}, ("g", k), ("gc", k))
        take(right, ("gr", k))
        send(right.at[:, HALF:], X.at[k, 2, :, HALF:], {"y": ym}, ("g", k), ("gh", k))
        send(right, X.at[k, 5], {"c": cc}, ("g", k), ("gc", k))

    def gather3(k):
        take(X.at[k, 2], ("gh", k))
        send(X.at[k, 2], X.at[k, 6], {"c": cc}, ("g", k), ("gc", k))

    def gather4(k):
        take(X.at[k, 4:8], ("gc", k))

    gather1(4)

    by_place = [jnp.where(own_quarter, dot(place_of, part), 0.0).astype(BF) for part in split(slot_weight)]
    sel_hi[...], sel_lo[...] = by_place

    def tile_row(a):
        return (((a >> 1) & 7) << 4) + ((a >> 5) << 2) + (((a >> 4) & 1) << 1) + (a & 1)

    def unpack_matrix():
        return ones_where(lane == tile_row(row))

    def pack_matrix():
        return ones_where(row == tile_row(lane))

    def unpack(k):
        take(tiles_of(rx, k), ("d", k))
        tiles = rx[8 * k : 8 * k + 8].reshape(128, 512)
        stacked = dot(unpack_matrix(), tiles).astype(BF)
        X[k, 0] = quarter_lanes(stacked, 32)

    def hidden_of(rows, gate_up):
        both = dot(rows, gate_up)
        gate = both[:, 0:128]
        return (gate * sigmoid(gate) * both[:, 128:256]).astype(BF)

    def experts(k):
        for j in range(2):
            rows = X[k, :, 16 * j : 16 * j + 16, :].reshape(128, 2048)
            hidden = hidden_of(rows, v_egu[j])
            Y[k, :, 16 * j : 16 * j + 16, :] = dot(hidden, v_ed[j]).astype(BF).reshape(8, 16, 2048)

    def shared_expert():
        rows = X[4].reshape(256, 2048)
        hidden = hidden_of(rows, v_sgu[...])
        Y[4] = dot(hidden, v_sd[...]).astype(BF).reshape(8, 32, 2048)

    def refs_of(k):
        if k == "a":
            return YA, PA, ZA, RAa, RBa, FAa, FDa, FBa, FEa, CAa, CBa
        return tuple(ref.at[k] for ref in (Y, PR, Z, RA, RB, FA, FD, FB, FE, CA, CB))

    def sum1(k):
        refs = refs_of(k)
        send(refs[0].at[4:8], refs[1], {"c": cc}, ("s", k), ("sp", k))

    def sum2(k):
        part, pair, total, ra, rb, fa, fd, fb, fe, ca, cb = refs_of(k)
        take(pair, ("sp", k))
        total[...] = (part[0:4].astype(F32) + pair[...].astype(F32)).astype(BF)
        send(total.at[2, :, 0:HALF], ra, {"y": yp}, ("s", k), ("sa", k))
        send(total.at[2, :, HALF:], rb, {"y": ym}, ("s", k), ("sb", k))
        send(total.at[1, :, HALF:], fe, {"y": yp}, ("s", k), ("sf", k))
        send(total.at[3, :, 0:HALF], fd, {"y": ym}, ("s", k), ("sf", k))

    def sum3(k):
        part, pair, total, ra, rb, fa, fd, fb, fe, ca, cb = refs_of(k)
        take(ra, ("sa", k))
        ca[...] = (total[1, :, 0:HALF].astype(F32) + ra[...].astype(F32)).astype(BF)
        send(ca, fa, {"y": yp}, ("s", k), ("sf", k))
        take(rb, ("sb", k))
        cb[...] = (total[3, :, HALF:].astype(F32) + rb[...].astype(F32)).astype(BF)
        send(cb, fb, {"y": ym}, ("s", k), ("sf", k))

    def sum4(k):
        part, pair, total, ra, rb, fa, fd, fb, fe, ca, cb = refs_of(k)
        take(total.at[0:2], ("sf", k))
        low = total[0, :, 0:HALF].astype(F32) + (fa[...].astype(F32) + fd[...].astype(F32))
        high = total[0, :, HALF:].astype(F32) + (fb[...].astype(F32) + fe[...].astype(F32))
        return jnp.concatenate([low, high], axis=1)

    def give_back(k):
        stacked = quarter_rows(sum4(k).astype(BF))
        packed = dot(pack_matrix(), stacked).astype(BF)
        rtx[8 * k : 8 * k + 8] = packed.reshape(8, 16, 512)
        for place in range(8 * k, 8 * k + 8):
            if place == OWN:
                rrx[OWN] = packed[0:16]
            else:
                send(rtx.at[place], rrx.at[place], source(place), "r", ("r", k))

    proj = {}

    def project():
        arrive("xa", "gain_a", "wq", "wk", "wv", "dd", "rd", "shift", "spike")
        arrive("decay_up", "decay_bias", "rate_up", "rate_base", "head_gain")
        normed = rms(v_xa[...], row_of(gain_a))
        qkv = dot(normed, v_qkv[...])
        last = ((1,), (1,))
        low = jnp.tanh(dot(normed, v_dd[...], last)).astype(BF)
        logits = decay_bias[...] + dot(low, decay_up[...]) + v_shift[...]
        log_decay = v_spike[...] - ROOT * sigmoid(logits)
        rate_low = dot(normed, v_rd[...], last).astype(BF)
        rate = sigmoid(rate_base[...] + dot(rate_low, rate_up[...]))
        q, k, v = qkv[:, 0:256], qkv[:, 256:512], qkv[:, 512:768]
        same = ones_where((iota((256, 256), 0) >> 6) == (iota((256, 256), 1) >> 6))
        unit = k * lax.rsqrt(dot_exact_right(k * k, same) + unit_eps)
        write = unit * rate
        block = (row >> 5) == (lane >> 5)
        cum = dot_exact_left(ones_where(block & (lane <= row)), log_decay)
        total = dot_exact_left(ones_where(block), log_decay)
        middle = 0.5 * total
        fade_in = jnp.exp(cum - middle)
        fade_out = jnp.exp(middle - cum)
        proj["qf"] = q * fade_in
        proj["ef"] = -unit * jnp.exp(cum - log_decay - middle)
        proj["wf"] = write * fade_out
        proj["kf"] = k * fade_out
        proj["v"] = v
        proj["em"] = jnp.exp(middle)
        proj["end"] = jnp.exp(total)

    def head(h):
        at = slice(HEAD * h, HEAD * h + HEAD)
        qf, ef, wf, kf, v, em, end = (proj[n][:, at] for n in ("qf", "ef", "wf", "kf", "v", "em", "end"))
        last = ((1,), (1,))
        block = (row >> 5) == (lane >> 5)
        strict, upto = block & (lane < row), block & (lane <= row)
        erase_write = jnp.where(strict, dot(ef, wf, last), 0.0)
        erase_key = jnp.where(strict, dot(ef, kf, last), 0.0)
        query_write = jnp.where(upto, dot(qf, wf, last), 0.0)
        query_key = jnp.where(upto, dot(qf, kf, last), 0.0)
        yield
        inverse = jnp.where(row == lane, 1.0, 0.0)
        for level in range(5):
            size = 1 << level
            corner = ((row >> (level + 1)) == (lane >> (level + 1))) & ((row & size) != 0) & ((lane & size) == 0)
            off = jnp.where(corner, erase_write, 0.0)
            if level == 0:
                inverse = inverse + off
            else:
                inverse = inverse + dot3(dot3(inverse, off), inverse)
                yield
        right = jnp.concatenate([ef * em, dot(erase_key, v)], axis=1)
        held = dot3(inverse, right)
        shown = dot(query_write, held) + jnp.concatenate([qf * em, dot(query_key, v)], axis=1)
        yield
        wide = (128, 256)
        mine_only = (iota(wide, 0) >> 5) == (iota(wide, 1) >> 6)
        ends_w = jnp.where(mine_only, jnp.concatenate([wf * em] * 4, axis=1), 0.0)
        ends_k = jnp.where(mine_only, jnp.concatenate([kf * em] * 4, axis=1), 0.0)
        ends = jnp.concatenate([ends_w, ends_k], axis=0)
        felt = jnp.concatenate([held, jnp.concatenate([jnp.zeros_like(v), v], axis=1)], axis=0)
        maps = dot(ends.T, felt)
        yield
        lane2, row2 = iota((HEAD, 128), 1), iota((HEAD, 128), 0)
        state = jnp.where(lane2 == row2, 1.0, 0.0)
        pieces = []
        for n in range(4):
            t = slice(SPAN * n, SPAN * n + SPAN)
            piece = dot3(shown[t, 0:HEAD], state)
            pieces.append(piece + jnp.where(iota((SPAN, 128), 1) >= HEAD, shown[t], 0.0))
            fade = jnp.concatenate([end[SPAN * n : SPAN * n + 1]] * 2, axis=1)
            step = maps[HEAD * n : HEAD * n + HEAD] + jnp.where(lane2 == row2, fade, 0.0)
            state = step if n == 0 else compose(step, state)
            yield
        umat[h] = jnp.concatenate(pieces, axis=0)
        atx[h] = state.astype(BF)
        yield

    walks = []

    def heads(steps):
        if not walks:
            walks.extend(head(h) for h in range(HEADS))
        for _ in range(steps):
            for walk in walks:
                next(walk)

    def scan1():
        arx[0] = atx[x]
        for d in range(1, 4):
            send(atx.at[(x + d) & 3], arx.at[d], {"x": (x + d) & 3}, "x", "x")

    def scan2():
        take(arx.at[1:4], "x")
        state = arx[x & 3].astype(F32)
        cmat[0] = state
        for n in range(1, 4):
            state = compose(arx[(x - n) & 3].astype(F32), state)
            cmat[n] = state
        ztx[...] = state.astype(BF)
        zrx[0] = ztx[...]
        for d in range(1, 8):
            send(ztx, zrx.at[d], {"z": (z + d) & 7}, "z", "z")

    def scan3():
        take(zrx.at[1:8], "z")
        lane2, row2 = iota((HEAD, 128), 1), iota((HEAD, 128), 0)
        state = jnp.where(lane2 == row2, 1.0, 0.0)
        for n in range(7):
            after = compose(zrx[(z - n) & 7].astype(F32), state)
            state = jnp.where(jnp.broadcast_to(n < z, after.shape), after, state)
        btx[0] = state.astype(BF)
        for n in range(1, 4):
            btx[n] = compose(cmat[n - 1], state).astype(BF)
        brx[0] = btx[x]
        for d in range(1, 4):
            send(btx.at[(x + d) & 3], brx.at[d], {"x": (x + d) & 3}, "b", "b")

    def finish_heads():
        take(brx.at[1:4], "b")
        outs = []
        for h in range(4):
            u = umat[h]
            outs.append((u + dot3(u[:, 0:HEAD], brx[(x - h) & 3].astype(F32)))[:, HEAD:])
        out = jnp.concatenate(outs, axis=1)
        same = ones_where((iota((256, 256), 0) >> 6) == (iota((256, 256), 1) >> 6))
        centered = out - dot_exact_right(out, same) * (1.0 / HEAD)
        var = dot_exact_right(centered * centered, same) * (1.0 / HEAD)
        mixed[...] = (centered * lax.rsqrt(var + group_eps) * row_of(head_gain).astype(F32)).astype(BF)

    def project_out():
        arrive("out")
        rows = jnp.concatenate(
            [
                mixed[pl.ds(pl.multiple_of(16 * (2 * ((y + r) & 3) + side), 16), 16), :]
                for side in (c, cc)
                for r in range(4)
            ],
            axis=0,
        )
        YA[...] = dot(rows, v_out[...]).astype(BF).reshape(8, 16, 2048)

    project()
    heads(2)
    gather2(4)
    unpack(0)
    gather1(0)
    heads(2)
    unpack(1)
    gather1(1)
    heads(1)
    gather2(0)
    heads(1)
    unpack(2)
    gather1(2)
    gather2(1)
    heads(1)
    unpack(3)
    gather1(3)
    heads(5)
    scan1()
    gather3(0)
    gather4(0)
    arrive("eg", "eu", "ed")
    experts(0)
    sum1(0)
    gather2(2)
    gather3(1)
    sum2(0)
    gather3(4)
    gather2(3)
    gather4(1)
    experts(1)
    sum1(1)
    scan2()
    gather3(2)
    sum2(1)
    sum3(0)
    gather4(2)
    experts(2)
    sum1(2)
    gather3(3)
    sum3(1)
    sum2(2)
    gather4(3)
    experts(3)
    sum1(3)
    gather4(4)
    arrive("sg", "su", "sd")
    shared_expert()
    sum1(4)
    give_back(0)
    scan3()
    sum3(2)
    sum2(3)
    give_back(1)
    finish_heads()
    project_out()
    sum1("a")
    sum3(3)
    sum2(4)
    give_back(2)
    sum2("a")
    sum3(4)
    give_back(3)
    sum3("a")
    total = sum4(4)
    out_a[...] = sum4("a").astype(BF)
    routed = None
    for k in range(CHUNKS):
        take(tiles_of(rrx, k), ("r", k))
        tiles = rrx[8 * k : 8 * k + 8].reshape(128, 512)
        at = slice(128 * k, 128 * k + 128)
        part = dot(sel_hi[at].T, tiles) + dot(sel_lo[at].T, tiles)
        routed = part if routed is None else routed + part
    out_b[...] = (quarter_lanes(routed, 32) + total).astype(BF)
    for k in range(5):
        sent(X.at[k, 0:7], ("g", k))
        sent(Y.at[k, 0:7], ("s", k))
    sent(YA.at[0:7], ("s", "a"))
    sent(atx.at[0:3], "x")
    sent(zrx.at[0:7], "z")
    sent(btx.at[0:3], "b")
    sent(tx.at[0:31], "d")
    sent(rtx.at[0:31], "r")
    assert (len(send_names), len(recv_names)) == (LEAVING, LANDING)


LEAVING, LANDING = 16, 55


def per_device(
    xa, gain_a, wq, wk, wv, decay_down, decay_up, decay_bias, decay_shift, decay_spike,
    rate_down, rate_up, rate_base, head_gain, w_out, xb, gain_b, ids, weights,
    e_gate, e_up, e_down, s_gate, s_up, s_down,
):
    here = pl.BlockSpec(memory_space=pltpu.VMEM)
    away = pl.BlockSpec(memory_space=pl.ANY)
    operands = [
        (xa, away), (gain_a, away), (wq, away), (wk, away), (wv, away),
        (decay_down.T, away), (decay_up, away), (decay_bias[None], away),
        (decay_shift, away), (decay_spike, away), (rate_down.T, away), (rate_up, away),
        (rate_base[None], away), (head_gain, away), (w_out, away), (xb, away),
        (gain_b, away), (ids.T, away), (weights.T, away), (e_gate, away), (e_up, away),
        (e_down, away), (s_gate, away), (s_up, away), (s_down, away),
    ]
    vm = pltpu.VMEM
    sums = lambda n: [
        vm((4, n, 2048), BF), vm((4, n, 2048), BF)] + [vm((n, HALF), BF)] * 8
    stacked = [vm((5,) + s.shape, BF) for s in sums(32)]
    scratch = [
        vm((128, 2048), BF), vm((2048, 768), BF), vm((64, 2048), BF), vm((64, 2048), BF),
        vm((128, 256), F32), vm((128, 256), F32), vm((256, 2048), BF), vm((2, 2048, 256), BF),
        vm((2, 128, 2048), BF), vm((2048, 256), BF), vm((128, 2048), BF),
        vm((2048,), BF), vm((64, 256), BF), vm((1, 256), F32), vm((64, 256), BF), vm((1, 256), F32),
        vm((256,), BF), vm((32, 2048), BF), vm((2048,), BF), vm((2, 256), jnp.int32), vm((2, 32), F32),
        vm((32, 16, 512), BF), vm((32, 16, 512), BF), vm((32, 16, 512), BF), vm((32, 16, 512), BF),
        vm((5, 8, 32, 2048), BF), vm((5, 8, 32, 2048), BF),
        *stacked,
        vm((8, 16, 2048), BF), *sums(16),
        vm((4, 64, 128), F32), vm((4, 128, 128), F32), vm((128, 256), BF),
        vm((4, 64, 128), BF), vm((4, 64, 128), BF), vm((64, 128), BF), vm((8, 64, 128), BF),
        vm((4, 64, 128), BF), vm((4, 64, 128), BF), vm((512, 128), BF), vm((512, 128), BF),
        pltpu.SemaphoreType.DMA((25,)), pltpu.SemaphoreType.DMA((LEAVING,)),
        pltpu.SemaphoreType.DMA((LANDING,)),
    ]
    return pl.pallas_call(
        kernel,
        out_shape=(vm((16, 2048), BF), vm((32, 2048), BF)),
        in_specs=[spec for _, spec in operands],
        out_specs=(here, here),
        scratch_shapes=scratch,
        compiler_params=pltpu.CompilerParams(
            collective_id=0, has_side_effects=True, vmem_limit_bytes=60 * 1024 * 1024
        ),
    )(*[array for array, _ in operands])


def solution(mesh):
    split_mesh = Mesh(mesh.devices.reshape(8, 4, 4, 2), ("z", "x", "y", "c"))
    ep, tp = ("z", "x"), ("y", "c")
    both = ep + tp
    return jax.shard_map(
        per_device,
        mesh=split_mesh,
        in_specs=(
            P(ep, None), P(), P(None, tp), P(None, tp), P(None, tp), P(), P(None, tp), P(tp),
            P(ep, tp), P(ep, tp), P(), P(None, tp), P(tp), P(tp), P(tp, None), P(both, None),
            P(), P(ep, None), P(both, None), P(ep, None, tp), P(ep, None, tp), P(ep, tp, None),
            P(None, tp), P(None, tp), P(tp, None),
        ),
        out_specs=(P(both, None), P(both, None)),
        check_vma=False,
    )
```
